128 devices in a mesh: sp: 32 (over z, y, core), tp: 4 (over x).
Axes of the slice: x: 4, y: 4, z: 4, core: 2. Of those that a mesh axis runs over, the one named last changes fastest.
Arguments:
- expert_input: bfloat16 [12288, 2048], P('sp'), may hold values from -6 to 6
- cotangent: bfloat16 [12288, 2048], P('sp'), may hold values from -6 to 6
- routes: int32 [12288, 2], P('sp'), may hold values from 0 to 31, all different within a row; in each aligned block of 384 rows (0 to 383, 384 to 767, ...) at most 36 rows name the same one
- route_weight: float32 [12288, 2], P('sp'), may hold values from 0.2 to 2.5
- expert_gate: bfloat16 [32, 2048, 1024], P('sp', None, 'tp'), may hold values from -0.125 to 0.125
- expert_up: bfloat16 [32, 2048, 1024], P('sp', None, 'tp'), may hold values from -0.125 to 0.125
- expert_down: bfloat16 [32, 1024, 2048], P('sp', 'tp'), may hold values from -0.1875 to 0.1875
- conv_out: bfloat16 [12288, 1024], P('sp', 'tp'), may hold values from -14 to 14
- conv_value: bfloat16 [12288, 1024], P('sp', 'tp'), may hold values from -6 to 6
- conv_gate: bfloat16 [12288, 1024], P('sp', 'tp'), may hold values from -6 to 6
- conv_taps: float32 [31, 1024], P(None, 'tp'), may hold values from -1 to 1
- norm_gain: float32 [1024], P('tp'), may hold values from 0.1 to 1.9
- norm_bias: float32 [1024], P('tp'), may hold values from -3 to 3
- out_weight: bfloat16 [1024, 2048], P('tp'), may hold values from -0.1875 to 0.1875
Outputs:
- gate_grad: float32 [32, 2048, 1024], P('sp', None, 'tp')
- up_grad: float32 [32, 2048, 1024], P('sp', None, 'tp')
- down_grad: float32 [32, 1024, 2048], P('sp', 'tp')
- resid_grad: bfloat16 [12288, 2048], P('sp')
- out_weight_grad: float32 [1024, 2048], P('tp', 'sp')
- value_grad: bfloat16 [12288, 1024], P('sp', 'tp')
- gate_in_grad: bfloat16 [12288, 1024], P('sp', 'tp')
The draws below stay inside these ranges and needn't reach their ends.
Inputs may be any that keep to these rules, and one draw needn't show every extreme that they name: `routes`: each token names 2 different experts. In each aligned block of 384 tokens no expert is named by more than 36 tokens, and in every draw some block has an expert named by exactly 36 tokens.
All inputs are finite; a program needn't handle non-finite values.
Results may differ from the reference program's by a relative error of at most 0.018.
Values may be sent and summed in bfloat16 or wider, within the bound.
A program may use at most 128 MiB of HBM per device.

```python
import math
import jax
import jax.numpy as jnp
import numpy as np
from jax import lax

D = 2048
CW = 1024
FF = 1024
KW = 31
TOP = 2
TOK_DEV = 384
TOKENS = 12288
EXPERTS = 32
CAP = 36
FGROUP = 256
N_SP = 32
N_TP = 4


def draw_conv_out(key, part):
    first_key = jax.random.fold_in(jax.random.fold_in(key, 11), 0)
    column = jnp.arange(CW, dtype=jnp.float32) / CW
    col_scale = 0.3 * jnp.exp(jnp.log(10.0) * column)[None, :]
    values = jnp.clip(jax.random.normal(first_key, (TOKENS, CW), jnp.float32), -4.0, 4.0) * col_scale
    return values.astype(jnp.bfloat16)


def spiked(array, rng, source, target, parts, factor):
    def block_of(axis_at):
        return (jnp.arange(array.shape[axis_at]) // (array.shape[axis_at] // parts)).reshape((-1,) + (1,) * (array.ndim - 1 - axis_at))

    near = jax.random.permutation(rng, parts)[block_of(target)]
    other_side = (block_of(target) + parts // 2) % parts
    return jnp.where((block_of(source) == near) | (block_of(source) == other_side), factor * array, array)


def levels(stream_key, dims, pieces, low, largest):
    loudness, own = 1.0, jax.random.fold_in(stream_key, 6)
    for position, parts in pieces:
        steps = jnp.exp(jax.random.uniform(jax.random.fold_in(own, position), (parts,), jnp.float32, low / len(pieces), largest / len(pieces)))
        loudness = loudness * jnp.repeat(steps, dims[position] // parts).reshape([-1 if axis == position else 1 for axis in range(len(dims))])
    return loudness


def assign_block(rng, own, number, rows, number_of, top, most, skew):
    order = jax.random.permutation(rng, number_of)
    crowded, usual = load_shares(number_of, rows * top, most, skew, True), load_shares(number_of, rows * top, most, skew, False)
    places = jnp.arange(number_of)

    def named(tallies, rotation):
        used = int((tallies > 0).sum())
        fixed = max(1, used // 4)
        moved = fixed + (places - fixed + rotation * (used - fixed)) % max(1, number_of - fixed)
        return jnp.zeros((number_of,), jnp.int32).at[order[jnp.where(places < fixed, places, moved)]].set(jnp.asarray(tallies, jnp.int32))

    tallies = jnp.where(number % 4 == 0, named(crowded, number // 4), named(usual, number - number // 4 - 1))
    mixed = jax.random.permutation(jax.random.fold_in(own, 3), number_of)
    donor, taker = mixed[0:number_of // 2 * 2:2], mixed[1:number_of // 2 * 2:2]
    slack = jnp.minimum(tallies[donor] - 1, most - tallies[taker]) // 2
    slack = jnp.where((donor == order[0]) | (taker == order[0]) | (tallies[taker] == 0), 0, jnp.maximum(slack, 0))
    moved = jax.random.randint(jax.random.fold_in(own, 4), (number_of // 2,), 0, 1 << 20) % (slack + 1)
    tallies = tallies.at[donor].add(-moved).at[taker].add(moved)
    items = jnp.searchsorted(jnp.cumsum(tallies), jnp.arange(rows * top), side="right").astype(jnp.int32)
    grid = items.reshape(top, rows).T
    grid = grid[jax.random.permutation(jax.random.fold_in(own, 1), rows)]
    rotation = jax.random.randint(jax.random.fold_in(own, 2), (rows, 1), 0, top)
    return jnp.take_along_axis(grid, (jnp.arange(top)[None, :] + rotation) % top, axis=1)


def load_shares(count, total, bound, slope, full):
    loads = [(1 << 20) // math.isqrt(grade ** slope) + 1 for grade in range(1, count + 1)]
    largest = bound if full else min(bound, max(-(-total // count), total * loads[0] // sum(loads)))
    least = 1 if total - largest >= count - 1 else 0
    holding, rest = [largest] + [least] * (count - 1), total - largest - least * (count - 1)
    while rest > 0:
        free = [i for i in range(1, count) if holding[i] < largest] or [i for i in range(1, count) if holding[i] < bound]
        mass, left = sum([loads[i] for i in free]), rest
        for i in free:
            addition = min(bound - holding[i], max(1, left * loads[i] // mass), rest)
            holding[i] = holding[i] + addition
            rest = rest - addition
    return np.array(holding)


def centred(rng, shape, width, most, pieces=(), kind=jnp.bfloat16):
    gain = levels(rng, shape, pieces, -0.22, 0.18) if pieces else 1.0
    entries = jax.random.normal(rng, shape, jnp.float32) * width * gain
    return jnp.minimum(jnp.maximum(entries, -most), most).astype(kind)


def noise_with(rng, shape, scale, limit, pieces, heavy, kind=jnp.bfloat16):
    entries = scale * jax.random.normal(rng, shape, jnp.float32)
    if pieces:
        entries = entries * levels(rng, shape, pieces, -0.22, 0.18)
    return jnp.clip(spiked(entries, jax.random.fold_in(rng, 3), *heavy), -limit, limit).astype(kind)


def setup_inputs(seed: int = 0) -> dict:
    key_list = jax.random.split(jax.random.key(seed), 15)
    expert_input = centred(key_list[0], (TOKENS, D), 1.0, 6.0, ((0, 32),))
    cotangent = noise_with(key_list[1], (TOKENS, D), 1.0, 6.0, ((0, 32),), (0, 1, 32, 2.75))
    routes_keys = jax.random.split(jax.random.fold_in(key_list[2], 1), TOKENS // TOK_DEV)
    routes_turns = jax.random.permutation(jax.random.fold_in(key_list[2], 3), TOKENS // TOK_DEV)
    routes = jax.vmap(lambda own, number: assign_block(jax.random.fold_in(key_list[2], 2), own, number, TOK_DEV, EXPERTS, TOP, CAP, 1))(routes_keys, routes_turns).reshape((TOKENS, TOP))
    route_weight = jnp.clip(jnp.exp(math.log(2.5) - 2.5257286 * jax.random.uniform(key_list[3], (TOKENS, TOP), jnp.float32) ** levels(key_list[3], (TOKENS, TOP), ((0, 32),), -0.2, 0.2)), 0.2, 2.5)
    expert_gate = centred(key_list[4], (EXPERTS, D, FF), D ** -0.5, 0.125, ((0, 32), (2, 4)))
    expert_up = centred(key_list[5], (EXPERTS, D, FF), D ** -0.5, 0.125, ((0, 32), (2, 4)))
    expert_down = centred(key_list[6], (EXPERTS, FF, D), FF ** -0.5, 0.1875, ((0, 32), (1, 4)))
    conv_out = draw_conv_out(jax.random.fold_in(key_list[14], 71), 0)
    conv_value = centred(key_list[8], (TOKENS, CW), 1.0, 6.0, ((0, 32), (1, 4)))
    conv_gate = centred(key_list[9], (TOKENS, CW), 1.0, 6.0, ((0, 32), (1, 4)))
    conv_taps = centred(key_list[10], (KW, CW), KW ** -0.5, 1.0, ((1, 4),), jnp.float32)
    norm_gain = jnp.clip(1.0 + 0.18 * jax.random.normal(key_list[11], (CW,), jnp.float32), 0.1, 1.9)
    norm_bias = centred(key_list[12], (CW,), 0.5, 3.0, ((0, 4),), jnp.float32)
    out_weight = centred(key_list[13], (CW, D), CW ** -0.5, 0.1875, ((0, 4),))
    return {"expert_input": expert_input, "cotangent": cotangent, "routes": routes, "route_weight": route_weight, "expert_gate": expert_gate, "expert_up": expert_up, "expert_down": expert_down, "conv_out": conv_out, "conv_value": conv_value, "conv_gate": conv_gate, "conv_taps": conv_taps, "norm_gain": norm_gain, "norm_bias": norm_bias, "out_weight": out_weight}


norm_eps = 1e-06

def build_slots(block_routes):
    assigns = block_routes.shape[0] * block_routes.shape[1]
    flat_routes = block_routes.reshape(assigns)
    onehot = (flat_routes[:, None] == jnp.arange(EXPERTS, dtype=jnp.int32)[None, :]).astype(jnp.int32)
    slot_rank = lax.optimization_barrier(jnp.sum((jnp.cumsum(onehot, axis=0) - onehot) * onehot, axis=1))
    target = flat_routes * CAP + slot_rank
    return jnp.full((EXPERTS * CAP,), assigns, jnp.int32).at[target].set(jnp.arange(assigns, dtype=jnp.int32))

def reference(expert_input, cotangent, routes, route_weight, expert_gate, expert_up, expert_down, conv_out, conv_value, conv_gate, conv_taps, norm_gain, norm_bias, out_weight):
    block_assigns = TOK_DEV * TOP
    slot_sets = jax.vmap(build_slots)(routes.reshape(N_SP, TOK_DEV, TOP))
    offsets = (jnp.arange(N_SP, dtype=jnp.int32) * block_assigns)[:, None]
    global_ids = jnp.where(slot_sets == block_assigns, TOKENS * TOP, slot_sets + offsets).astype(jnp.int32)
    expert_ids = global_ids.reshape(N_SP, EXPERTS, CAP).transpose(1, 0, 2).reshape(EXPERTS, N_SP * CAP)
    scaled = (cotangent.astype(jnp.float32)[:, None, :] * route_weight[:, :, None]).astype(jnp.bfloat16)
    padded_cot = jnp.concatenate([scaled.reshape(TOKENS * TOP, D), jnp.zeros((1, D), jnp.bfloat16)], axis=0)
    padded_in = jnp.concatenate([expert_input, jnp.zeros((1, D), jnp.bfloat16)], axis=0)

    def expert_step(routed, inputs):
        slot_ids, w_gate, w_up, w_down = inputs
        tokens_of = slot_ids // TOP
        slot_rows = padded_in[tokens_of]
        slot_cots = padded_cot[slot_ids]
        pre_gate = jnp.dot(slot_rows, w_gate, preferred_element_type=jnp.float32)
        pre_up = jnp.dot(slot_rows, w_up, preferred_element_type=jnp.float32)
        gate_sig = jax.nn.sigmoid(pre_gate)
        gate_act = pre_gate * gate_sig
        hidden = (gate_act * pre_up).astype(jnp.bfloat16)
        hidden_grad = jnp.dot(slot_cots, w_down.T, preferred_element_type=jnp.float32)
        down_part = jnp.dot(hidden.T, slot_cots, preferred_element_type=jnp.float32)
        gate_pre = (hidden_grad * pre_up * gate_sig * (1.0 + pre_gate * (1.0 - gate_sig))).astype(jnp.bfloat16)
        up_pre = (hidden_grad * gate_act).astype(jnp.bfloat16)
        gate_part = jnp.dot(slot_rows.T, gate_pre, preferred_element_type=jnp.float32)
        up_part = jnp.dot(slot_rows.T, up_pre, preferred_element_type=jnp.float32)
        slot_grad = jnp.zeros((slot_rows.shape[0], D), jnp.float32)
        for group_idx in range(N_TP):
            group_lo = group_idx * FGROUP
            group_hi = group_lo + FGROUP
            group_part = jnp.dot(gate_pre[:, group_lo:group_hi], w_gate[:, group_lo:group_hi].T, preferred_element_type=jnp.float32)
            group_part = group_part + jnp.dot(up_pre[:, group_lo:group_hi], w_up[:, group_lo:group_hi].T, preferred_element_type=jnp.float32)
            slot_grad = slot_grad + lax.optimization_barrier(group_part.astype(jnp.bfloat16)).astype(jnp.float32)
        rounded = lax.optimization_barrier(slot_grad.astype(jnp.bfloat16)).astype(jnp.float32)
        routed = routed.at[tokens_of].add(rounded)
        return (routed, (gate_part, up_part, down_part))
    routed, weight_grads = lax.scan(expert_step, jnp.zeros((TOKENS + 1, D), jnp.float32), (expert_ids, expert_gate, expert_up, expert_down))
    gate_grad, up_grad, down_grad = weight_grads
    resid_grad = (cotangent.astype(jnp.float32) + routed[:TOKENS]).astype(jnp.bfloat16)
    mix_grad = jnp.dot(resid_grad, out_weight.T, preferred_element_type=jnp.float32)
    conv_vals = conv_out.astype(jnp.float32)
    row_mean = lax.optimization_barrier(jnp.mean(conv_vals, axis=1, keepdims=True))
    row_var = lax.optimization_barrier(jnp.mean((conv_vals - row_mean) ** 2, axis=1, keepdims=True))
    row_rstd = lax.rsqrt(row_var + norm_eps)
    normed = (conv_vals - row_mean) * row_rstd
    norm_pre = normed * norm_gain[None, :] + norm_bias[None, :]
    norm_sig = jax.nn.sigmoid(norm_pre)
    conv_act = (norm_pre * norm_sig).astype(jnp.bfloat16)
    out_weight_grad = jnp.dot(conv_act.T, resid_grad, preferred_element_type=jnp.float32)
    norm_grad = mix_grad * norm_sig * (1.0 + norm_pre * (1.0 - norm_sig)) * norm_gain[None, :]
    grad_mean = lax.optimization_barrier(jnp.mean(norm_grad, axis=1, keepdims=True))
    grad_dot = lax.optimization_barrier(jnp.mean(norm_grad * normed, axis=1, keepdims=True))
    conv_grad = row_rstd * (norm_grad - grad_mean - normed * grad_dot)
    extended = jnp.concatenate([conv_grad, jnp.zeros((KW - 1, CW), jnp.float32)], axis=0)
    glu_grad = jnp.zeros((TOKENS, CW), jnp.float32)
    for lag_index in range(KW):
        begin = KW - 1 - lag_index
        glu_grad = glu_grad + conv_taps[lag_index][None, :] * extended[begin:begin + TOKENS]
    gate_sig = jax.nn.sigmoid(conv_gate.astype(jnp.float32))
    value_grad = (glu_grad * gate_sig).astype(jnp.bfloat16)
    gate_in_grad = (glu_grad * conv_value.astype(jnp.float32) * gate_sig * (1.0 - gate_sig)).astype(jnp.bfloat16)
    return (gate_grad, up_grad, down_grad, resid_grad, out_weight_grad, value_grad, gate_in_grad)
```

```python
import jax
import jax.numpy as jnp
from jax import lax
from jax.experimental import pallas as pl
from jax.experimental.pallas import tpu as pltpu
from jax.sharding import PartitionSpec as P

MESH = pl.DeviceIdType.MESH
bf16 = jnp.bfloat16
f32 = jnp.float32
norm_eps = 1e-06

NSP = 32
NTP = 4
ROWS = 384
D = 2048
QW = 512
FG = 256
GRP = 8
GR = 288
NT = 9


def dot(a, b, ca=1, cb=0):
    return lax.dot_general(a, b, (((ca,), (cb,)), ((), ())), preferred_element_type=f32)


def iota(shape, dim):
    return lax.broadcasted_iota(jnp.int32, shape, dim)


def moe_kernel(
    x_ref,
    c_ref,
    routes_ref,
    weight_ref,
    wg_ref,
    wu_ref,
    wd_ref,
    gg_ref,
    ug_ref,
    dg_ref,
    resid_ref,
    rank_ref,
    wsel_ref,
    ohm_ref,
    ohr_ref,
    send_ref,
    got_ref,
    rows_ref,
    hid_ref,
    part_ref,
    pair_ref,
    back_ref,
    home_ref,
    flat_ref,
    flatr_ref,
    exo_ref,
    exi_ref,
    ag_ref,
    fsend,
    frecv,
    xfsend,
    xfrecv,
    xbsend,
    xbrecv,
    bsend,
    brecv,
    esend,
    erecv,
    asend,
    arecv,
):
    me = lax.axis_index("sp")
    x = lax.axis_index("tp")
    z, y, core = me // 8, (me // 2) % 4, me % 2
    right, left = (x + 1) % NTP, (x + 3) % NTP

    def peer_at(dz, m):
        return ((z + dz) % 4) * 8 + ((y + m // 2) % 4) * 2 + (core + m % 2) % 2

    def source_at(dz, m):
        return ((z + 4 - dz) % 4) * 8 + ((y + 4 - m // 2) % 4) * 2 + (core + m % 2) % 2

    def quarter(j):
        return (x + j) % NTP

    barrier = pltpu.get_barrier_semaphore()

    @pl.loop(1, NSP)
    def _(k):
        pl.semaphore_signal(
            barrier, inc=1, device_id=(peer_at(k // 8, k % 8), x), device_id_type=MESH
        )

    for side in (left, right):
        pl.semaphore_signal(barrier, inc=1, device_id=(me, side), device_id_type=MESH)

    r0, r1 = routes_ref[0:1, :], routes_ref[1:2, :]
    names = iota((NSP, ROWS), 0)
    m0, m1 = r0 == names, r1 == names
    member = jnp.where(m0 | m1, 1.0, 0.0).astype(bf16)
    before = jnp.where(iota((ROWS, ROWS), 0) < iota((ROWS, ROWS), 1), 1.0, 0.0).astype(bf16)
    rank = dot(member, before)
    rank_ref[...] = jnp.where(m0 | m1, rank, -1.0).astype(jnp.int32)
    wsel_ref[...] = jnp.where(m0, weight_ref[0:1, :], jnp.where(m1, weight_ref[1:2, :], 0.0))

    @pl.loop(0, NSP // GRP)
    def _(g):
        ranks = rank_ref[pl.ds(pl.multiple_of(g * GRP, GRP), GRP), :]
        wsel = wsel_ref[pl.ds(pl.multiple_of(g * GRP, GRP), GRP), :]
        ohs, ws, ohrs, wrs = [], [], [], []
        for i in range(GRP):
            one = ranks[i : i + 1] == iota((32, ROWS), 0)
            ohs.append(jnp.where(one, 1.0, 0.0).astype(bf16))
            ws.append(jnp.sum(jnp.where(one, wsel[i : i + 1], 0.0), axis=1, keepdims=True))
            one = ranks[i : i + 1] == 32 + iota((16, ROWS), 0) % 4
            ohrs.append(jnp.where(one, 1.0, 0.0).astype(bf16))
            wrs.append(jnp.sum(jnp.where(one, wsel[i : i + 1], 0.0), axis=1, keepdims=True))
        oh = jnp.concatenate(ohs, axis=0)
        ohr = jnp.concatenate(ohrs, axis=0)
        ohm_ref[pl.ds(pl.multiple_of(g * 256, 256), 256), :] = oh
        ohr_ref[pl.ds(pl.multiple_of(g * 128, 128), 128), :] = ohr
        w = jnp.concatenate(ws, axis=0)
        wr = jnp.concatenate(wrs, axis=0)
        col = (iota((128, 128), 0) % 16) // 4
        for t in range(2):
            for j in range(2):
                ref = c_ref if t else x_ref
                src = ref[:, pl.ds(pl.multiple_of(quarter(j) * QW, QW), QW)]
                main = dot(oh, src)
                rem = dot(ohr, src)
                if t:
                    main = main * w
                    rem = rem * wr
                main = main.astype(bf16)
                tail = jnp.zeros((128, 128), f32)
                for cg in range(4):
                    tail = jnp.where(col == cg, rem[:, cg * 128 : (cg + 1) * 128], tail)
                tail = tail.astype(bf16)
                for i in range(GRP):
                    for rt in range(2):
                        for ct in range(4):
                            send_ref[t, g * GRP + i, j, rt * 4 + ct] = main[
                                i * 32 + rt * 16 : i * 32 + rt * 16 + 16, ct * 128 : ct * 128 + 128
                            ]
                    send_ref[t, g * GRP + i, j, 8] = tail[i * 16 : i * 16 + 16]

    pl.semaphore_wait(barrier, NSP - 1 + 2)

    def forward_copy(t, k):
        peer = peer_at(k // 8, k % 8)
        return pltpu.make_async_remote_copy(
            src_ref=send_ref.at[t, peer],
            dst_ref=got_ref.at[t, me, 0:2],
            send_sem=fsend.at[t],
            recv_sem=frecv.at[t, k],
            device_id=(peer, x),
            device_id_type=MESH,
        )

    @pl.loop(0, 4)
    def _(dz):
        for t in range(2):

            @pl.loop(0, 8)
            def _(m):
                @pl.when(dz + m > 0)
                def _():
                    forward_copy(t, dz * 8 + m).start()

    for t in range(2):
        got_ref[t, me, 0:2] = send_ref[t, me]

    def to_side(src, t, origin, dz, side):
        return pltpu.make_async_remote_copy(
            src_ref=src,
            dst_ref=got_ref.at[t, origin, 2 + side],
            send_sem=xfsend.at[side],
            recv_sem=xfrecv.at[dz, side],
            device_id=(me, right if side else left),
            device_id_type=MESH,
        )

    def pass_on(dz):
        for t in range(2):

            @pl.loop(0, 8)
            def _(m):
                k = dz * 8 + m
                origin = source_at(dz, m)

                @pl.when(k > 0)
                def _():
                    pltpu.make_async_remote_copy(
                        src_ref=send_ref.at[t, origin],
                        dst_ref=got_ref.at[t, origin, 0:2],
                        send_sem=fsend.at[t],
                        recv_sem=frecv.at[t, k],
                        device_id=(origin, x),
                        device_id_type=MESH,
                    ).wait_recv()
                    to_side(got_ref.at[t, origin, 0], t, origin, dz, 1).start()
                    to_side(got_ref.at[t, origin, 1], t, origin, dz, 0).start()

                @pl.when(k == 0)
                def _():
                    to_side(send_ref.at[t, origin, 0], t, origin, dz, 1).start()
                    to_side(send_ref.at[t, origin, 1], t, origin, dz, 0).start()

    a = iota((128, 128), 0)
    perm_col = (a % 32) // 4 * 16 + (a // 32) * 4 + a % 4
    perm = jnp.where(iota((128, 128), 1) == perm_col, 1.0, 0.0).astype(bf16)

    def experts(dz):
        zs = (z + 4 - dz) % 4
        base = zs * GR
        first = zs * 8
        for side in range(2):
            whole = got_ref.at[:, pl.ds(first, 8), 2 + side]
            pltpu.make_async_remote_copy(
                src_ref=whole,
                dst_ref=whole,
                send_sem=xfsend.at[side],
                recv_sem=xfrecv.at[dz, side],
                device_id=(me, right if side else left),
                device_id_type=MESH,
            ).wait_recv()
        for t in range(2):
            for r in range(4):
                lane = quarter(r) * QW

                @pl.loop(0, 8)
                def _(i):
                    for rt in range(2):
                        for ct in range(4):
                            rows_ref[
                                t,
                                pl.ds(pl.multiple_of(base + i * 32 + rt * 16, 16), 16),
                                pl.ds(pl.multiple_of(lane + ct * 128, 128), 128),
                            ] = got_ref[t, first + i, r, rt * 4 + ct]

                rem = dot(perm, got_ref[t, pl.ds(first, 8), r, 8].reshape(128, 128)).astype(bf16)
                for cg in range(4):
                    rows_ref[
                        t,
                        pl.ds(pl.multiple_of(base + 256, 16), 32),
                        pl.ds(pl.multiple_of(lane + cg * 128, 128), 128),
                    ] = rem[cg * 32 : cg * 32 + 32]
        span = pl.ds(pl.multiple_of(base, 32), GR)
        tok = rows_ref[0, span, :]
        pre_gate = dot(tok, wg_ref[...])
        pre_up = dot(tok, wu_ref[...])
        hidden_grad = dot(rows_ref[1, span, :], wd_ref[...], 1, 1)
        sig = jax.nn.sigmoid(pre_gate)
        act = pre_gate * sig
        hid_ref[0, span, :] = (act * pre_up).astype(bf16)
        gate_pre = (hidden_grad * pre_up * sig * (1.0 + pre_gate * (1.0 - sig))).astype(bf16)
        up_pre = (hidden_grad * act).astype(bf16)
        hid_ref[1, span, :] = gate_pre
        hid_ref[2, span, :] = up_pre
        for r in (2, 3, 0, 1):
            cols = pl.ds(pl.multiple_of(quarter(r) * QW, QW), QW)
            part = dot(gate_pre, wg_ref[cols, :], 1, 1) + dot(up_pre, wu_ref[cols, :], 1, 1)
            part = part.astype(bf16)
            for i in range(8):
                for rt in range(2):
                    for ct in range(4):
                        part_ref[r, first + i, rt * 4 + ct] = part[
                            i * 32 + rt * 16 : i * 32 + rt * 16 + 16, ct * 128 : ct * 128 + 128
                        ]
            stack = jnp.concatenate(
                [part[256:GR, cg * 128 : cg * 128 + 128] for cg in range(4)], axis=0
            )
            rem = dot(perm, stack, 0, 0).astype(bf16)
            for i in range(8):
                part_ref[r, first + i, 8] = rem[i * 16 : i * 16 + 16]
            if r == 3:
                for side in range(2):
                    pair_copy(dz, side).start()

    def pair_copy(dz, side):
        group = pl.ds(((z + 4 - dz) % 4) * 8, 8)
        return pltpu.make_async_remote_copy(
            src_ref=part_ref.at[3 - side, group],
            dst_ref=pair_ref.at[side, group],
            send_sem=xbsend.at[dz, side],
            recv_sem=xbrecv.at[dz, side],
            device_id=(me, right if side else left),
            device_id_type=MESH,
        )

    def back_copy(dz, m):
        origin = source_at(dz, m)
        return pltpu.make_async_remote_copy(
            src_ref=back_ref.at[origin],
            dst_ref=home_ref.at[me],
            send_sem=bsend.at[dz],
            recv_sem=brecv.at[dz],
            device_id=(origin, x),
            device_id_type=MESH,
        )

    def send_back(dz):
        for side in range(2):
            pair_copy(dz, side).wait_recv()

        @pl.loop(0, 8)
        def _(m):
            origin = source_at(dz, m)
            for j in range(2):
                both = part_ref[j, origin].astype(f32) + pair_ref[j, origin].astype(f32)
                back_ref[origin, j] = both.astype(bf16)

        @pl.loop(0, 8)
        def _(m):
            @pl.when(dz + m > 0)
            def _():
                back_copy(dz, m).start()

            @pl.when(dz + m == 0)
            def _():
                home_ref[me] = back_ref[me]

    @pl.loop(0, 6)
    def _(step):
        @pl.when(step < 4)
        def _():
            pass_on(step)

        @pl.when((step > 0) & (step < 5))
        def _():
            experts(step - 1)

        @pl.when(step > 1)
        def _():
            send_back(step - 2)

    @pl.loop(0, 4)
    def _(g):
        cols = pl.ds(pl.multiple_of(g * QW, QW), QW)
        tok = rows_ref[0, :, cols]
        gg_ref[cols, :] = dot(tok, hid_ref[1], 0, 0)
        ug_ref[cols, :] = dot(tok, hid_ref[2], 0, 0)
        dg_ref[:, cols] = dot(hid_ref[0], rows_ref[1, :, cols], 0, 0)

    for dz in range(4):
        group = pl.ds(((z + dz) % 4) * 8, 8)
        span = home_ref.at[pl.ds(0, 7)] if dz == 0 else home_ref.at[group]
        pltpu.make_async_remote_copy(
            src_ref=span,
            dst_ref=span,
            send_sem=bsend.at[dz],
            recv_sem=brecv.at[dz],
            device_id=(peer_at(1, 0), x),
            device_id_type=MESH,
        ).wait_recv()

    @pl.loop(0, NSP)
    def _(e):
        for j in range(2):
            for rt in range(2):
                for ct in range(4):
                    flat_ref[
                        pl.ds(pl.multiple_of(e * 32 + rt * 16, 16), 16),
                        pl.ds(j * QW + ct * 128, 128),
                    ] = home_ref[e, j, rt * 4 + ct]
            flatr_ref[pl.ds(pl.multiple_of(e * 16, 16), 16), pl.ds(j * 128, 128)] = home_ref[e, j, 8]

    rem_group = (iota((512, 1), 0) % 16) // 4
    sums = []
    for j in range(2):
        main = dot(ohm_ref[...], flat_ref[:, j * QW : (j + 1) * QW], 0, 0)
        tails = []
        for cg in range(4):
            tail = jnp.where(
                rem_group == cg, flatr_ref[:, j * 128 : (j + 1) * 128].astype(f32), 0.0
            ).astype(bf16)
            tails.append(tail)
        tail = dot(ohr_ref[...], jnp.concatenate(tails, axis=1), 0, 0)
        sums.append(main + tail)
    exo_ref[0] = sums[0][:, 256:].astype(bf16)
    exo_ref[1] = sums[1][:, :256].astype(bf16)

    def exchange(side):
        return pltpu.make_async_remote_copy(
            src_ref=exo_ref.at[side],
            dst_ref=exi_ref.at[side],
            send_sem=esend.at[side],
            recv_sem=erecv.at[side],
            device_id=(me, right if side else left),
            device_id_type=MESH,
        )

    for side in range(2):
        exchange(side).start()
    for side in range(2):
        exchange(side).wait_recv()
    cot0 = c_ref[:, pl.ds(pl.multiple_of(quarter(0) * QW, 256), 256)].astype(f32)
    cot1 = c_ref[:, pl.ds(pl.multiple_of(quarter(1) * QW + 256, 256), 256)].astype(f32)
    ag_ref[0, 0] = (cot0 + (sums[0][:, :256] + exi_ref[1].astype(f32))).astype(bf16)
    ag_ref[0, 1] = (cot1 + (sums[1][:, 256:] + exi_ref[0].astype(f32))).astype(bf16)

    def gather(side):
        return pltpu.make_async_remote_copy(
            src_ref=ag_ref.at[0],
            dst_ref=ag_ref.at[3 if side else 1],
            send_sem=asend.at[side],
            recv_sem=arecv.at[side],
            device_id=(me, right if side else left),
            device_id_type=MESH,
        )

    def gather_far(side):
        return pltpu.make_async_remote_copy(
            src_ref=ag_ref.at[3 if side else 1, 1 - side],
            dst_ref=ag_ref.at[2, 1 - side],
            send_sem=asend.at[2 + side],
            recv_sem=arecv.at[2 + side],
            device_id=(me, right if side else left),
            device_id_type=MESH,
        )

    def place(o):
        resid_ref[:, pl.ds(pl.multiple_of(quarter(o) * QW, 256), 256)] = ag_ref[o, 0]
        resid_ref[:, pl.ds(pl.multiple_of(quarter(o + 1) * QW + 256, 256), 256)] = ag_ref[o, 1]

    for side in range(2):
        gather(side).start()
    place(0)
    for side in range(2):
        gather(side).wait_recv()
        gather_far(side).start()
    place(1)
    place(3)
    for side in range(2):
        gather_far(side).wait_recv()
    place(2)

    for side in range(2):
        exchange(side).wait_send()
        gather(side).wait_send()
        gather_far(side).wait_send()
        whole = got_ref.at[:, :, side]
        pltpu.make_async_remote_copy(
            src_ref=whole,
            dst_ref=whole,
            send_sem=xfsend.at[side],
            recv_sem=xfrecv.at[0, side],
            device_id=(me, right if side else left),
            device_id_type=MESH,
        ).wait_send()
        for dz in range(4):
            pair_copy(dz, side).wait_send()
    for t in range(2):
        whole = send_ref.at[t, pl.ds(0, NSP - 1)]
        pltpu.make_async_remote_copy(
            src_ref=whole,
            dst_ref=whole,
            send_sem=fsend.at[t],
            recv_sem=frecv.at[t, 0],
            device_id=(peer_at(1, 0), x),
            device_id_type=MESH,
        ).wait_send()
    for dz in range(4):
        span = back_ref.at[pl.ds(0, 7 if dz == 0 else 8)]
        pltpu.make_async_remote_copy(
            src_ref=span,
            dst_ref=span,
            send_sem=bsend.at[dz],
            recv_sem=brecv.at[dz],
            device_id=(peer_at(1, 0), x),
            device_id_type=MESH,
        ).wait_send()


def moe(expert_input, cotangent, routes, route_weight, wg, wu, wd):
    dma = pltpu.SemaphoreType.DMA
    vmem = pl.BlockSpec(memory_space=pltpu.VMEM)
    return pl.pallas_call(
        moe_kernel,
        out_shape=(
            jax.ShapeDtypeStruct((D, FG), f32),
            jax.ShapeDtypeStruct((D, FG), f32),
            jax.ShapeDtypeStruct((FG, D), f32),
            jax.ShapeDtypeStruct((ROWS, D), bf16),
        ),
        in_specs=[vmem] * 7,
        out_specs=(vmem,) * 4,
        scratch_shapes=[
            pltpu.VMEM((NSP, ROWS), jnp.int32),
            pltpu.VMEM((NSP, ROWS), f32),
            pltpu.VMEM((1024, ROWS), bf16),
            pltpu.VMEM((512, ROWS), bf16),
            pltpu.VMEM((2, NSP, 2, NT, 16, 128), bf16),
            pltpu.VMEM((2, NSP, 4, NT, 16, 128), bf16),
            pltpu.VMEM((2, 4 * GR, D), bf16),
            pltpu.VMEM((3, 4 * GR, FG), bf16),
            pltpu.VMEM((4, NSP, NT, 16, 128), bf16),
            pltpu.VMEM((2, NSP, NT, 16, 128), bf16),
            pltpu.VMEM((NSP, 2, NT, 16, 128), bf16),
            pltpu.VMEM((NSP, 2, NT, 16, 128), bf16),
            pltpu.VMEM((1024, 1024), bf16),
            pltpu.VMEM((512, 256), bf16),
            pltpu.VMEM((2, ROWS, 256), bf16),
            pltpu.VMEM((2, ROWS, 256), bf16),
            pltpu.VMEM((4, 2, ROWS, 256), bf16),
            dma((2,)),
            dma((2, NSP)),
            dma((2,)),
            dma((4, 2)),
            dma((4, 2)),
            dma((4, 2)),
            dma((4,)),
            dma((4,)),
            dma((2,)),
            dma((2,)),
            dma((4,)),
            dma((4,)),
        ],
        compiler_params=pltpu.CompilerParams(
            collective_id=0, has_side_effects=True, vmem_limit_bytes=66000000
        ),
        name="moe",
    )(expert_input, cotangent, routes.T, route_weight.T, wg, wu, wd)


def passed_along(value, axis, steps):
    count = lax.axis_size(axis)
    leading, last = (max(0, -steps), min(count, count - steps))
    return lax.ppermute(value, axis, [(source, source + steps) for source in range(leading, last)])


def cut_along(x, dim, size):
    lengths = x.shape
    tiles = x.reshape(*lengths[:dim], size, lengths[dim] // size, *lengths[dim + 1 :])
    return jnp.moveaxis(tiles, dim, 0)


def sent_and_summed(x, axis, dim):
    size = lax.axis_size(axis)
    tiles = lax.all_to_all(cut_along(x, dim, size), axis, 0, 0, tiled=True)
    return jnp.sum(tiles.astype(jnp.float32), axis=0)


def on_device(
    expert_input,
    cotangent,
    routes,
    route_weight,
    expert_gate,
    expert_up,
    expert_down,
    conv_out,
    conv_value,
    conv_gate,
    conv_taps,
    norm_gain,
    norm_bias,
    out_weight,
):
    tp_count = lax.axis_size("tp")
    tok_rows, model_width = expert_input.shape
    gate_grad, up_grad, down_grad, resid_grad = moe(
        expert_input, cotangent, routes, route_weight, expert_gate[0], expert_up[0], expert_down[0]
    )
    gate_grad, up_grad, down_grad = gate_grad[None], up_grad[None], down_grad[None]
    mix_grad = lax.dot_general(
        resid_grad, out_weight, (((1,), (1,)), ((), ())), preferred_element_type=jnp.float32
    )
    channels = conv_out.shape[1] * tp_count
    conv_vals = conv_out.astype(jnp.float32)
    row_sum, row_square = lax.psum(
        (jnp.sum(conv_vals, axis=1), jnp.sum(conv_vals * conv_vals, axis=1)), "tp"
    )
    row_mean = (row_sum / channels)[:, None]
    row_var = (row_square / channels)[:, None] - row_mean * row_mean
    row_rstd = lax.rsqrt(row_var + norm_eps)
    normed = (conv_vals - row_mean) * row_rstd
    norm_pre = normed * norm_gain[None, :] + norm_bias[None, :]
    norm_sig = jax.nn.sigmoid(norm_pre)
    conv_act = (norm_pre * norm_sig).astype(jnp.bfloat16)
    norm_grad = mix_grad * norm_sig * (1.0 + norm_pre * (1.0 - norm_sig)) * norm_gain[None, :]
    grad_sum, grad_dot = lax.psum(
        (jnp.sum(norm_grad, axis=1), jnp.sum(norm_grad * normed, axis=1)), "tp"
    )
    conv_grad = row_rstd * (
        norm_grad - (grad_sum / channels)[:, None] - normed * (grad_dot / channels)[:, None]
    )
    taps_count = conv_taps.shape[0]
    next_rows = passed_along(conv_grad[: taps_count - 1], "sp", -1)
    extended = jnp.concatenate([conv_grad, next_rows], axis=0)
    glu_grad = jnp.zeros_like(conv_grad)
    for lag_index in range(taps_count):
        begin = taps_count - 1 - lag_index
        glu_grad = glu_grad + conv_taps[lag_index][None, :] * extended[begin : begin + tok_rows]
    gate_sig_in = jax.nn.sigmoid(conv_gate.astype(jnp.float32))
    value_grad = (glu_grad * gate_sig_in).astype(jnp.bfloat16)
    gate_in_grad = (
        glu_grad * conv_value.astype(jnp.float32) * gate_sig_in * (1.0 - gate_sig_in)
    ).astype(jnp.bfloat16)
    projected = sent_and_summed(
        lax.dot_general(
            resid_grad, conv_act, (((0,), (0,)), ((), ())), preferred_element_type=jnp.float32
        ).astype(jnp.bfloat16),
        "sp",
        0,
    )
    out_weight_grad = projected.T
    return (gate_grad, up_grad, down_grad, resid_grad, out_weight_grad, value_grad, gate_in_grad)


def solution(mesh):
    return jax.shard_map(
        on_device,
        mesh=mesh,
        in_specs=(
            P("sp", None),
            P("sp", None),
            P("sp", None),
            P("sp", None),
            P("sp", None, "tp"),
            P("sp", None, "tp"),
            P("sp", "tp", None),
            P("sp", "tp"),
            P("sp", "tp"),
            P("sp", "tp"),
            P(None, "tp"),
            P("tp"),
            P("tp"),
            P("tp", None),
        ),
        out_specs=(
            P("sp", None, "tp"),
            P("sp", None, "tp"),
            P("sp", "tp", None),
            P("sp", None),
            P("tp", "sp"),
            P("sp", "tp"),
            P("sp", "tp"),
        ),
        check_vma=False,
    )
```

```python
import jax
import jax.numpy as jnp
from jax import lax
from jax.experimental import pallas as pl
from jax.experimental.pallas import tpu as pltpu
from jax.sharding import PartitionSpec as P

MESH = pl.DeviceIdType.MESH
bf16 = jnp.bfloat16
f32 = jnp.float32
norm_eps = 1e-06

NSP = 32
NTP = 4
ROWS = 384
D = 2048
CH = 1024
KW = 31
QW = 512
FG = 256
NG = 8
GB = NSP // NG
GR = GB * 36
GM = GB * 32
GT = GB * 16
NT = 9
OW = D // NSP


def dot(a, b, ca=1, cb=0, precision=None):
    return lax.dot_general(
        a, b, (((ca,), (cb,)), ((), ())), preferred_element_type=f32, precision=precision
    )


def exact_dot(a, b, ca=1, cb=0):
    return dot(a, b, ca, cb, lax.Precision.HIGHEST)


def iota(shape, dim):
    return lax.broadcasted_iota(jnp.int32, shape, dim)


def at(start, size, step):
    return pl.ds(pl.multiple_of(start, step), size)


def layer_kernel(
    x_hbm,
    c_hbm,
    wg_hbm,
    wu_hbm,
    wd_hbm,
    ow_hbm,
    co_hbm,
    cv_hbm,
    cg_hbm,
    routes_ref,
    weight_ref,
    taps_ref,
    gain_ref,
    bias_ref,
    gg_hbm,
    ug_hbm,
    dg_hbm,
    resid_hbm,
    owg_ref,
    value_ref,
    gatein_ref,
    x_ref,
    c_ref,
    wg_ref,
    wu_ref,
    wd_ref,
    ow_ref,
    co_ref,
    cv_ref,
    cg_ref,
    gg_ref,
    ug_ref,
    dg_ref,
    resid_ref,
    rank_ref,
    wsel_ref,
    ohm_ref,
    ohr_ref,
    send_ref,
    got_ref,
    rows_ref,
    hid_ref,
    part_ref,
    pair_ref,
    back_ref,
    home_ref,
    flat_ref,
    flatr_ref,
    exo_ref,
    exi_ref,
    ag_ref,
    stat_ref,
    normed_ref,
    coef_ref,
    rstd_ref,
    act_ref,
    ext_ref,
    halo_ref,
    pso_ref,
    psi_ref,
    insem,
    outsem,
    fsend,
    frecv,
    xfsend,
    xfrecv,
    xbsend,
    xbrecv,
    bsend,
    brecv,
    esend,
    erecv,
    asend,
    arecv,
    ssend,
    srecv,
    hsend,
    hrecv,
    psend,
    precv,
):
    me = lax.axis_index("sp")
    x = lax.axis_index("tp")
    z, y, core = me // 8, (me // 2) % 4, me % 2
    right, left = (x + 1) % NTP, (x + 3) % NTP

    def offset(k):
        g, m = k // GB, k % GB
        lap, part = g * 4 // NG, g % (NG // 4)
        dz = part + (m // 2) * (NG // 4)
        return dz, (dz + lap) % 4, m % 2

    def peer_at(k):
        dz, dy, dc = offset(k)
        return ((z + dz) % 4) * 8 + ((y + dy) % 4) * 2 + (core + dc) % 2

    def source_at(k):
        dz, dy, dc = offset(k)
        return ((z + 4 - dz) % 4) * 8 + ((y + 4 - dy) % 4) * 2 + (core + dc) % 2

    def quarter(j):
        return (x + j) % NTP

    def remote(src, dst, send, recv, sp, tp):
        return pltpu.make_async_remote_copy(
            src_ref=src,
            dst_ref=dst,
            send_sem=send,
            recv_sem=recv,
            device_id=(sp, tp),
            device_id_type=MESH,
        )

    def to_left_or_right(side):
        return right if side else left

    loads = [
        pltpu.make_async_copy(src, dst, insem.at[n])
        for n, (src, dst) in enumerate(
            [
                (x_hbm, x_ref),
                (c_hbm, c_ref),
                (wg_hbm, wg_ref),
                (wu_hbm, wu_ref),
                (wd_hbm, wd_ref),
                (co_hbm, co_ref),
                (ow_hbm, ow_ref),
                (cv_hbm, cv_ref),
                (cg_hbm, cg_ref),
            ]
        )
    ]
    for load in loads:
        load.start()

    barrier = pltpu.get_barrier_semaphore()

    @pl.loop(1, NSP)
    def _(k):
        pl.semaphore_signal(barrier, inc=1, device_id=(peer_at(k), x), device_id_type=MESH)

    for j in range(1, NTP):
        pl.semaphore_signal(barrier, inc=1, device_id=(me, quarter(j)), device_id_type=MESH)

    r0, r1 = routes_ref[0:1, :], routes_ref[1:2, :]
    names = iota((NSP, ROWS), 0)
    m0, m1 = r0 == names, r1 == names
    member = jnp.where(m0 | m1, 1.0, 0.0).astype(bf16)
    before = jnp.where(iota((ROWS, ROWS), 0) < iota((ROWS, ROWS), 1), 1.0, 0.0).astype(bf16)
    rank = dot(member, before)
    rank_ref[...] = jnp.where(m0 | m1, rank, -1.0).astype(jnp.int32)
    wsel_ref[...] = jnp.where(m0, weight_ref[0:1, :], jnp.where(m1, weight_ref[1:2, :], 0.0))
    loads[0].wait()
    loads[1].wait()

    def forward_copy(t, k, peer):
        return remote(
            send_ref.at[t, k], got_ref.at[t, k, 0:2], fsend.at[t], frecv.at[t, k], peer, x
        )

    tile_col = (iota((GT, 128), 0) % 16) // 4

    @pl.loop(0, NG)
    def _(g):
        ohs, ws, ohrs, wrs = [], [], [], []
        for i in range(GB):
            peer = peer_at(g * GB + i)
            ranks = rank_ref[pl.ds(peer, 1), :]
            wsel = wsel_ref[pl.ds(peer, 1), :]
            one = ranks == iota((32, ROWS), 0)
            ohs.append(jnp.where(one, 1.0, 0.0).astype(bf16))
            ws.append(jnp.sum(jnp.where(one, wsel, 0.0), axis=1, keepdims=True))
            one = ranks == 32 + iota((16, ROWS), 0) % 4
            ohrs.append(jnp.where(one, 1.0, 0.0).astype(bf16))
            wrs.append(jnp.sum(jnp.where(one, wsel, 0.0), axis=1, keepdims=True))
        oh = jnp.concatenate(ohs, axis=0)
        ohr = jnp.concatenate(ohrs, axis=0)
        ohm_ref[at(g * GM, GM, GM), :] = oh
        ohr_ref[at(g * GT, GT, GT), :] = ohr
        w = jnp.concatenate(ws, axis=0)
        wr = jnp.concatenate(wrs, axis=0)
        for t in range(2):
            for j in range(2):
                ref = c_ref if t else x_ref
                src = ref[:, at(quarter(j) * QW, QW, QW)]
                main = dot(oh, src)
                rem = dot(ohr, src)
                if t:
                    main = main * w
                    rem = rem * wr
                main = main.astype(bf16)
                tail = jnp.zeros((GT, 128), f32)
                for cg in range(4):
                    tail = jnp.where(tile_col == cg, rem[:, cg * 128 : (cg + 1) * 128], tail)
                tail = tail.astype(bf16)
                for i in range(GB):
                    for rt in range(2):
                        for ct in range(4):
                            send_ref[t, g * GB + i, j, rt * 4 + ct] = main[
                                i * 32 + rt * 16 : i * 32 + rt * 16 + 16, ct * 128 : ct * 128 + 128
                            ]
                    send_ref[t, g * GB + i, j, 8] = tail[i * 16 : i * 16 + 16]

        @pl.when(g == 0)
        def _():
            pl.semaphore_wait(barrier, NSP - 1 + NTP - 1)

        for t in range(2):
            for i in range(GB):
                k = g * GB + i

                @pl.when(k > 0)
                def _():
                    forward_copy(t, k, peer_at(k)).start()

    for t in range(2):
        got_ref[t, 0, 0:2] = send_ref[t, 0]

    for load in loads[2:]:
        load.wait()
    ones = jnp.ones((8, FG), f32)
    spread = jnp.where(iota((8, 128), 0) == 0, 1.0, 0.0)
    spread1 = jnp.where(iota((8, 128), 0) == 1, 1.0, 0.0)

    def stat_copy(n, j):
        return remote(
            stat_ref.at[n, 0], stat_ref.at[n, NTP - j], ssend.at[n], srecv.at[n], me, quarter(j)
        )

    def stat_start(n, rows):
        stat_ref[n, 0] = rows
        for j in range(1, NTP):
            stat_copy(n, j).start()

    def stat_total(n):
        whole = stat_ref.at[n, pl.ds(1, NTP - 1)]
        remote(whole, whole, ssend.at[n], srecv.at[n], me, right).wait_recv()
        return (stat_ref[n, 0] + stat_ref[n, 1]) + (stat_ref[n, 2] + stat_ref[n, 3])

    def column(row_form, pick):
        one = exact_dot(row_form, pick, 0, 0)
        return jnp.concatenate([one, one], axis=1)

    stat_start(0, exact_dot(ones, co_ref[...].astype(f32), 1, 1))

    def to_side(src, t, k, side):
        return remote(
            src,
            got_ref.at[t, k, 2 + side],
            xfsend.at[side],
            xfrecv.at[k // GB, side],
            me,
            to_left_or_right(side),
        )

    def pass_on(g):
        for t in range(2):

            @pl.loop(0, GB)
            def _(m):
                k = g * GB + m

                @pl.when(k > 0)
                def _():
                    forward_copy(t, k, source_at(k)).wait_recv()
                    to_side(got_ref.at[t, k, 0], t, k, 1).start()
                    to_side(got_ref.at[t, k, 1], t, k, 0).start()

                @pl.when(k == 0)
                def _():
                    to_side(send_ref.at[t, k, 0], t, k, 1).start()
                    to_side(send_ref.at[t, k, 1], t, k, 0).start()

    a = iota((GT, GT), 0)
    perm_col = (a % (GB * 4)) // 4 * 16 + (a // (GB * 4)) * 4 + a % 4
    perm = jnp.where(iota((GT, GT), 1) == perm_col, 1.0, 0.0).astype(bf16)

    def experts(g):
        base = g * GR
        first = g * GB
        for side in range(2):
            whole = got_ref.at[:, pl.ds(first, GB), 2 + side]
            remote(
                whole, whole, xfsend.at[side], xfrecv.at[g, side], me, to_left_or_right(side)
            ).wait_recv()
        for t in range(2):
            for r in range(4):
                lane = quarter(r) * QW
                for i in range(GB):
                    for rt in range(2):
                        for ct in range(4):
                            rows_ref[
                                t,
                                at(base + i * 32 + rt * 16, 16, 16),
                                at(lane + ct * 128, 128, 128),
                            ] = got_ref[t, first + i, r, rt * 4 + ct]
                rem = dot(perm, got_ref[t, pl.ds(first, GB), r, 8].reshape(GT, 128)).astype(bf16)
                for cg in range(4):
                    rows_ref[
                        t, at(base + GM, GB * 4, 16), at(lane + cg * 128, 128, 128)
                    ] = rem[cg * GB * 4 : (cg + 1) * GB * 4]
        span = at(base, GR, 16)
        tok = rows_ref[0, span, :]
        pre_gate = dot(tok, wg_ref[...])
        pre_up = dot(tok, wu_ref[...])
        hidden_grad = dot(rows_ref[1, span, :], wd_ref[...], 1, 1)
        sig = jax.nn.sigmoid(pre_gate)
        act = pre_gate * sig
        hid_ref[0, span, :] = (act * pre_up).astype(bf16)
        gate_pre = (hidden_grad * pre_up * sig * (1.0 + pre_gate * (1.0 - sig))).astype(bf16)
        up_pre = (hidden_grad * act).astype(bf16)
        hid_ref[1, span, :] = gate_pre
        hid_ref[2, span, :] = up_pre
        for r in (2, 3, 0, 1):
            cols = at(quarter(r) * QW, QW, QW)
            part = dot(gate_pre, wg_ref[cols, :], 1, 1) + dot(up_pre, wu_ref[cols, :], 1, 1)
            part = part.astype(bf16)
            for i in range(GB):
                for rt in range(2):
                    for ct in range(4):
                        part_ref[r, first + i, rt * 4 + ct] = part[
                            i * 32 + rt * 16 : i * 32 + rt * 16 + 16, ct * 128 : ct * 128 + 128
                        ]
            stack = jnp.concatenate(
                [part[GM:GR, cg * 128 : cg * 128 + 128] for cg in range(4)], axis=0
            )
            rem = dot(perm, stack, 0, 0).astype(bf16)
            for i in range(GB):
                part_ref[r, first + i, 8] = rem[i * 16 : i * 16 + 16]
            if r >= 2:
                pair_copy(g, 3 - r).start()

    def pair_copy(g, side):
        group = pl.ds(g * GB, GB)
        return remote(
            part_ref.at[3 - side, group],
            pair_ref.at[side, group],
            xbsend.at[g, side],
            xbrecv.at[g, side],
            me,
            to_left_or_right(side),
        )

    def back_copy(g, m):
        k = g * GB + m
        return remote(
            back_ref.at[k], home_ref.at[k], bsend.at[g], brecv.at[g], source_at(k), x
        )

    def send_back(g):
        for side in range(2):
            pair_copy(g, side).wait_recv()

        @pl.loop(0, GB)
        def _(m):
            k = g * GB + m
            for j in range(2):
                both = part_ref[j, k].astype(f32) + pair_ref[j, k].astype(f32)
                back_ref[k, j] = both.astype(bf16)

            @pl.when(k > 0)
            def _():
                back_copy(g, m).start()

            @pl.when(k == 0)
            def _():
                home_ref[0] = back_ref[0]

    @pl.loop(0, NG + 2)
    def _(step):
        @pl.when(step < NG)
        def _():
            pass_on(step)

        @pl.when((step > 0) & (step <= NG))
        def _():
            experts(step - 1)

        @pl.when(step > 1)
        def _():
            send_back(step - 2)

    @pl.loop(0, 4)
    def _(g):
        cols = at(g * QW, QW, QW)
        tok = rows_ref[0, :, cols]
        gg_ref[cols, :] = dot(tok, hid_ref[1], 0, 0).astype(bf16)
        ug_ref[cols, :] = dot(tok, hid_ref[2], 0, 0).astype(bf16)
        dg_ref[:, cols] = dot(hid_ref[0], rows_ref[1, :, cols], 0, 0).astype(bf16)

    stores = [
        pltpu.make_async_copy(src, dst, outsem.at[n])
        for n, (src, dst) in enumerate(
            [(gg_ref, gg_hbm), (ug_ref, ug_hbm), (dg_ref, dg_hbm), (resid_ref, resid_hbm)]
        )
    ]
    for store in stores[:3]:
        store.start()

    conv = co_ref[...].astype(f32)
    mean = column(stat_total(0), spread) / CH
    centred = conv - mean
    stat_start(1, exact_dot(ones, centred * centred, 1, 1))
    var = column(stat_total(1), spread) / CH
    rstd = lax.rsqrt(var + norm_eps)
    normed = centred * rstd
    norm_pre = normed * gain_ref[...] + bias_ref[...]
    norm_sig = jax.nn.sigmoid(norm_pre)
    act_ref[...] = (norm_pre * norm_sig).astype(bf16)
    normed_ref[...] = normed
    rstd_ref[...] = rstd
    coef_ref[...] = norm_sig * (1.0 + norm_pre * (1.0 - norm_sig)) * gain_ref[...]

    for g in range(NG):
        span = home_ref.at[pl.ds(1, GB - 1)] if g == 0 else home_ref.at[pl.ds(g * GB, GB)]
        remote(span, span, bsend.at[g], brecv.at[g], peer_at(1), x).wait_recv()

    @pl.loop(0, NSP)
    def _(e):
        for j in range(2):
            for rt in range(2):
                for ct in range(4):
                    flat_ref[at(e * 32 + rt * 16, 16, 16), pl.ds(j * QW + ct * 128, 128)] = (
                        home_ref[e, j, rt * 4 + ct]
                    )
            flatr_ref[at(e * 16, 16, 16), pl.ds(j * 128, 128)] = home_ref[e, j, 8]

    rem_group = (iota((512, 1), 0) % 16) // 4
    sums = []
    for j in range(2):
        main = dot(ohm_ref[...], flat_ref[:, j * QW : (j + 1) * QW], 0, 0)
        rems = flatr_ref[:, j * 128 : (j + 1) * 128].astype(f32)
        tails = [jnp.where(rem_group == cg, rems, 0.0).astype(bf16) for cg in range(4)]
        sums.append(main + dot(ohr_ref[...], jnp.concatenate(tails, axis=1), 0, 0))
    exo_ref[0] = sums[0][:, 256:].astype(bf16)
    exo_ref[1] = sums[1][:, :256].astype(bf16)

    def exchange(side):
        return remote(
            exo_ref.at[side],
            exi_ref.at[side],
            esend.at[side],
            erecv.at[side],
            me,
            to_left_or_right(side),
        )

    for side in range(2):
        exchange(side).start()
    for side in range(2):
        exchange(side).wait_recv()
    cot0 = c_ref[:, at(quarter(0) * QW, 256, 256)].astype(f32)
    cot1 = c_ref[:, at(quarter(1) * QW + 256, 256, 256)].astype(f32)
    ag_ref[0, 0] = (cot0 + (sums[0][:, :256] + exi_ref[1].astype(f32))).astype(bf16)
    ag_ref[0, 1] = (cot1 + (sums[1][:, 256:] + exi_ref[0].astype(f32))).astype(bf16)

    def gather(side):
        return remote(
            ag_ref.at[0],
            ag_ref.at[3 if side else 1],
            asend.at[side],
            arecv.at[side],
            me,
            to_left_or_right(side),
        )

    def gather_far(side):
        return remote(
            ag_ref.at[3 if side else 1, 1 - side],
            ag_ref.at[2, 1 - side],
            asend.at[2 + side],
            arecv.at[2 + side],
            me,
            to_left_or_right(side),
        )

    def place(o):
        resid_ref[:, at(quarter(o) * QW, 256, 256)] = ag_ref[o, 0]
        resid_ref[:, at(quarter(o + 1) * QW + 256, 256, 256)] = ag_ref[o, 1]

    for side in range(2):
        gather(side).start()
    place(0)
    for side in range(2):
        gather(side).wait_recv()
        gather_far(side).start()
    place(1)
    place(3)
    for side in range(2):
        gather_far(side).wait_recv()
    place(2)
    stores[3].start()

    mix_grad = dot(resid_ref[...], ow_ref[...], 1, 1)
    norm_grad = mix_grad * coef_ref[...]
    sum_rows = exact_dot(ones, norm_grad, 1, 1)
    dot_rows = exact_dot(ones, norm_grad * normed_ref[...], 1, 1)
    stat_start(2, jnp.where(iota((8, ROWS), 0) == 0, sum_rows, dot_rows))

    def owg_copy(k, peer):
        return remote(pso_ref.at[k], psi_ref.at[k], psend.at[0], precv.at[0], peer, x)

    @pl.loop(0, 4)
    def _(g):
        cols = at(g * QW, QW, QW)
        term = dot(resid_ref[:, cols], act_ref[...], 0, 0).astype(bf16)
        for i in range(8):
            for rt in range(4):
                for ct in range(2):
                    flat_ref[
                        at((g % 2) * 512 + i * OW + rt * 16, 16, 16),
                        at((g // 2) * 256 + ct * 128, 128, 128),
                    ] = term[i * OW + rt * 16 : i * OW + rt * 16 + 16, ct * 128 : ct * 128 + 128]

    @pl.loop(0, NSP)
    def _(k):
        peer = peer_at(k)
        for rt in range(4):
            for ct in range(2):
                pso_ref[k, rt * 2 + ct] = flat_ref[
                    at((peer % 16) * OW + rt * 16, 16, 16),
                    at((peer // 16) * 256 + ct * 128, 128, 128),
                ]

        @pl.when(k > 0)
        def _():
            owg_copy(k, peer).start()

    totals = stat_total(2)
    conv_grad = rstd_ref[...] * (
        norm_grad
        - column(totals, spread) / CH
        - normed_ref[...] * (column(totals, spread1) / CH)
    )
    ext_ref[0:ROWS, :] = conv_grad

    def halo_copy(sp):
        return remote(ext_ref.at[0:32], halo_ref, hsend.at[0], hrecv.at[0], sp, x)

    @pl.when(me > 0)
    def _():
        halo_copy(me - 1).start()

    def convolve(start, rows):
        glu = jnp.zeros((rows, FG), f32)
        for lag in range(KW):
            begin = start + KW - 1 - lag
            glu = glu + taps_ref[lag : lag + 1, :] * ext_ref[begin : begin + rows, :]
        span = pl.ds(start, rows)
        gate_sig = jax.nn.sigmoid(cg_ref[span, :].astype(f32))
        value_ref[span, :] = (glu * gate_sig).astype(bf16)
        gatein_ref[span, :] = (
            glu * cv_ref[span, :].astype(f32) * gate_sig * (1.0 - gate_sig)
        ).astype(bf16)

    for start in range(0, ROWS - 32, 32):
        convolve(start, 32)

    @pl.when(me < NSP - 1)
    def _():
        halo_copy(me + 1).wait_recv()
        ext_ref[ROWS : ROWS + 32, :] = halo_ref[...]

    @pl.when(me == NSP - 1)
    def _():
        ext_ref[ROWS : ROWS + 32, :] = jnp.zeros((32, FG), f32)

    convolve(ROWS - 32, 32)

    whole = psi_ref.at[pl.ds(1, NSP - 1)]
    remote(whole, whole, psend.at[0], precv.at[0], me, right).wait_recv()
    for rt in range(4):
        for ct in range(2):
            total = pso_ref[0, rt * 2 + ct].astype(f32)
            for k in range(1, NSP):
                total = total + psi_ref[k, rt * 2 + ct].astype(f32)
            owg_ref[rt * 16 : rt * 16 + 16, ct * 128 : ct * 128 + 128] = total

    @pl.when(me > 0)
    def _():
        halo_copy(me - 1).wait_send()

    remote(whole, whole, psend.at[0], precv.at[0], me, right).wait_send()
    for n in range(3):
        sent = stat_ref.at[n, pl.ds(1, NTP - 1)]
        remote(sent, sent, ssend.at[n], srecv.at[n], me, right).wait_send()
    for side in range(2):
        exchange(side).wait_send()
        gather(side).wait_send()
        gather_far(side).wait_send()
        sent = got_ref.at[:, :, side]
        remote(sent, sent, xfsend.at[side], xfrecv.at[0, side], me, right).wait_send()
        for g in range(NG):
            pair_copy(g, side).wait_send()
    for t in range(2):
        sent = send_ref.at[t, pl.ds(0, NSP - 1)]
        remote(sent, sent, fsend.at[t], frecv.at[t, 0], me, right).wait_send()
    for g in range(NG):
        sent = back_ref.at[pl.ds(0, GB - 1 if g == 0 else GB)]
        remote(sent, sent, bsend.at[g], brecv.at[g], me, right).wait_send()
    for store in stores:
        store.wait()


def on_device(
    expert_input,
    cotangent,
    routes,
    route_weight,
    expert_gate,
    expert_up,
    expert_down,
    conv_out,
    conv_value,
    conv_gate,
    conv_taps,
    norm_gain,
    norm_bias,
    out_weight,
):
    dma = pltpu.SemaphoreType.DMA
    vmem = pl.BlockSpec(memory_space=pltpu.VMEM)
    anywhere = pl.BlockSpec(memory_space=pl.ANY)
    shape = jax.ShapeDtypeStruct
    gate_grad, up_grad, down_grad, resid_grad, projected, value_grad, gate_in_grad = pl.pallas_call(
        layer_kernel,
        out_shape=(
            shape((D, FG), bf16),
            shape((D, FG), bf16),
            shape((FG, D), bf16),
            shape((ROWS, D), bf16),
            shape((OW, FG), f32),
            shape((ROWS, FG), bf16),
            shape((ROWS, FG), bf16),
        ),
        in_specs=[anywhere] * 9 + [vmem] * 5,
        out_specs=(anywhere,) * 4 + (vmem,) * 3,
        scratch_shapes=[
            pltpu.VMEM((ROWS, D), bf16),
            pltpu.VMEM((ROWS, D), bf16),
            pltpu.VMEM((D, FG), bf16),
            pltpu.VMEM((D, FG), bf16),
            pltpu.VMEM((FG, D), bf16),
            pltpu.VMEM((FG, D), bf16),
            pltpu.VMEM((ROWS, FG), bf16),
            pltpu.VMEM((ROWS, FG), bf16),
            pltpu.VMEM((ROWS, FG), bf16),
            pltpu.VMEM((D, FG), bf16),
            pltpu.VMEM((D, FG), bf16),
            pltpu.VMEM((FG, D), bf16),
            pltpu.VMEM((ROWS, D), bf16),
            pltpu.VMEM((NSP, ROWS), jnp.int32),
            pltpu.VMEM((NSP, ROWS), f32),
            pltpu.VMEM((1024, ROWS), bf16),
            pltpu.VMEM((512, ROWS), bf16),
            pltpu.VMEM((2, NSP, 2, NT, 16, 128), bf16),
            pltpu.VMEM((2, NSP, 4, NT, 16, 128), bf16),
            pltpu.VMEM((2, NSP * 36, D), bf16),
            pltpu.VMEM((3, NSP * 36, FG), bf16),
            pltpu.VMEM((4, NSP, NT, 16, 128), bf16),
            pltpu.VMEM((2, NSP, NT, 16, 128), bf16),
            pltpu.VMEM((NSP, 2, NT, 16, 128), bf16),
            pltpu.VMEM((NSP, 2, NT, 16, 128), bf16),
            pltpu.VMEM((1024, 1024), bf16),
            pltpu.VMEM((512, 256), bf16),
            pltpu.VMEM((2, ROWS, 256), bf16),
            pltpu.VMEM((2, ROWS, 256), bf16),
            pltpu.VMEM((4, 2, ROWS, 256), bf16),
            pltpu.VMEM((3, NTP, 8, ROWS), f32),
            pltpu.VMEM((ROWS, FG), f32),
            pltpu.VMEM((ROWS, FG), f32),
            pltpu.VMEM((ROWS, FG), f32),
            pltpu.VMEM((ROWS, FG), bf16),
            pltpu.VMEM((ROWS + 32, FG), f32),
            pltpu.VMEM((32, FG), f32),
            pltpu.VMEM((NSP, 8, 16, 128), bf16),
            pltpu.VMEM((NSP, 8, 16, 128), bf16),
            dma((9,)),
            dma((4,)),
            dma((2,)),
            dma((2, NSP)),
            dma((2,)),
            dma((NG, 2)),
            dma((NG, 2)),
            dma((NG, 2)),
            dma((NG,)),
            dma((NG,)),
            dma((2,)),
            dma((2,)),
            dma((4,)),
            dma((4,)),
            dma((3,)),
            dma((3,)),
            dma((1,)),
            dma((1,)),
            dma((1,)),
            dma((1,)),
        ],
        compiler_params=pltpu.CompilerParams(
            collective_id=0, has_side_effects=True, vmem_limit_bytes=67000000
        ),
        name="layer",
    )(
        expert_input,
        cotangent,
        expert_gate[0],
        expert_up[0],
        expert_down[0],
        out_weight,
        conv_out,
        conv_value,
        conv_gate,
        routes.T,
        route_weight.T,
        conv_taps,
        norm_gain[None, :],
        norm_bias[None, :],
    )
    return (
        gate_grad[None].astype(f32),
        up_grad[None].astype(f32),
        down_grad[None].astype(f32),
        resid_grad,
        projected.T,
        value_grad,
        gate_in_grad,
    )


def solution(mesh):
    return jax.shard_map(
        on_device,
        mesh=mesh,
        in_specs=(
            P("sp", None),
            P("sp", None),
            P("sp", None),
            P("sp", None),
            P("sp", None, "tp"),
            P("sp", None, "tp"),
            P("sp", "tp", None),
            P("sp", "tp"),
            P("sp", "tp"),
            P("sp", "tp"),
            P(None, "tp"),
            P("tp"),
            P("tp"),
            P("tp", None),
        ),
        out_specs=(
            P("sp", None, "tp"),
            P("sp", None, "tp"),
            P("sp", "tp", None),
            P("sp", None),
            P("tp", "sp"),
            P("sp", "tp"),
            P("sp", "tp"),
        ),
        check_vma=False,
    )
```

```python
import jax
import jax.numpy as jnp
from jax import lax
from jax.experimental import pallas as pl
from jax.experimental.pallas import tpu as pltpu
from jax.sharding import PartitionSpec as P

MESH = pl.DeviceIdType.MESH
bf16 = jnp.bfloat16
f32 = jnp.float32
norm_eps = 1e-06

NSP = 32
NTP = 4
ROWS = 384
D = 2048
CH = 1024
KW = 31
QW = 512
FG = 256
NG = 8
GB = NSP // NG
GR = GB * 36
GM = GB * 32
GT = GB * 16
GO = GM + GT
NT = 9
WHOLE = 2
OW = D // NSP


def dot(a, b, ca=1, cb=0, precision=None):
    return lax.dot_general(
        a, b, (((ca,), (cb,)), ((), ())), preferred_element_type=f32, precision=precision
    )


def exact_dot(a, b, ca=1, cb=0):
    return dot(a, b, ca, cb, lax.Precision.HIGHEST)


def iota(shape, dim):
    return lax.broadcasted_iota(jnp.int32, shape, dim)


def at(start, size, step):
    return pl.ds(pl.multiple_of(start, step), size)


def layer_kernel(
    x_hbm,
    c_hbm,
    wg_hbm,
    wu_hbm,
    wd_hbm,
    ow_hbm,
    co_hbm,
    cv_hbm,
    cg_hbm,
    routes_ref,
    weight_ref,
    taps_ref,
    gain_ref,
    bias_ref,
    gg_hbm,
    ug_hbm,
    dg_hbm,
    resid_hbm,
    owg_ref,
    value_ref,
    gatein_ref,
    x_ref,
    c_ref,
    wg_ref,
    wu_ref,
    wd_ref,
    ow_ref,
    co_ref,
    cv_ref,
    cg_ref,
    gg_ref,
    ug_ref,
    dg_ref,
    resid_ref,
    rank_ref,
    wsel_ref,
    oh_ref,
    send_ref,
    more_ref,
    got_ref,
    rows_ref,
    hid_ref,
    part_ref,
    pair_ref,
    back_ref,
    home_ref,
    sum_ref,
    exo_ref,
    exi_ref,
    ag_ref,
    stat_ref,
    normed_ref,
    coef_ref,
    rstd_ref,
    act_ref,
    ext_ref,
    halo_ref,
    pso_ref,
    psi_ref,
    insem,
    outsem,
    fsend,
    frecv,
    msend,
    mrecv,
    xfsend,
    xfrecv,
    xbsend,
    xbrecv,
    bsend,
    brecv,
    esend,
    erecv,
    asend,
    arecv,
    ssend,
    srecv,
    hsend,
    hrecv,
    psend,
    precv,
):
    me = lax.axis_index("sp")
    x = lax.axis_index("tp")
    z, y, core = me // 8, (me // 2) % 4, me % 2
    right, left = (x + 1) % NTP, (x + 3) % NTP

    def offset(k):
        g, m = k // GB, k % GB
        lap, part = g * 4 // NG, g % (NG // 4)
        dz = part + (m // 2) * (NG // 4)
        return dz, (dz + lap) % 4, m % 2

    def peer_at(k):
        dz, dy, dc = offset(k)
        return ((z + dz) % 4) * 8 + ((y + dy) % 4) * 2 + (core + dc) % 2

    def source_at(k):
        dz, dy, dc = offset(k)
        return ((z + 4 - dz) % 4) * 8 + ((y + 4 - dy) % 4) * 2 + (core + dc) % 2

    def quarter(j):
        return (x + j) % NTP

    def remote(src, dst, send, recv, sp, tp):
        return pltpu.make_async_remote_copy(
            src_ref=src,
            dst_ref=dst,
            send_sem=send,
            recv_sem=recv,
            device_id=(sp, tp),
            device_id_type=MESH,
        )

    def to_left_or_right(side):
        return right if side else left

    loads = [
        pltpu.make_async_copy(src, dst, insem.at[n])
        for n, (src, dst) in enumerate(
            [
                (x_hbm, x_ref),
                (c_hbm, c_ref),
                (wg_hbm, wg_ref),
                (wu_hbm, wu_ref),
                (wd_hbm, wd_ref),
                (co_hbm, co_ref),
                (ow_hbm, ow_ref),
                (cv_hbm, cv_ref),
                (cg_hbm, cg_ref),
            ]
        )
    ]
    for load in loads:
        load.start()

    barrier = pltpu.get_barrier_semaphore()

    @pl.loop(1, NSP)
    def _(k):
        pl.semaphore_signal(barrier, inc=1, device_id=(peer_at(k), x), device_id_type=MESH)

    for j in range(1, NTP):
        pl.semaphore_signal(barrier, inc=1, device_id=(me, quarter(j)), device_id_type=MESH)

    r0, r1 = routes_ref[0:1, :], routes_ref[1:2, :]
    names = iota((NSP, ROWS), 0)
    m0, m1 = r0 == names, r1 == names
    member = jnp.where(m0 | m1, 1.0, 0.0).astype(bf16)
    before = jnp.where(iota((ROWS, ROWS), 0) < iota((ROWS, ROWS), 1), 1.0, 0.0).astype(bf16)
    rank = dot(member, before)
    rank_ref[...] = jnp.where(m0 | m1, rank, -1.0).astype(jnp.int32)
    wsel_ref[...] = jnp.where(m0, weight_ref[0:1, :], jnp.where(m1, weight_ref[1:2, :], 0.0))
    loads[0].wait()
    loads[1].wait()

    def forward_copy(t, k, peer):
        return remote(
            send_ref.at[t, k], got_ref.at[t, k, 0:2], fsend.at[t], frecv.at[t, k], peer, x
        )

    def more_copy(t, slot, k, peer):
        return remote(
            more_ref.at[t, slot], got_ref.at[t, k, 2:4], msend.at[0], mrecv.at[t, slot], peer, x
        )

    tile_col = (iota((GT, 128), 0) % 16) // 4

    def prepare(g):
        ohs, ws, ohrs, wrs = [], [], [], []
        for i in range(GB):
            peer = peer_at(g * GB + i)
            ranks = rank_ref[pl.ds(peer, 1), :]
            wsel = wsel_ref[pl.ds(peer, 1), :]
            one = ranks == iota((32, ROWS), 0)
            ohs.append(jnp.where(one, 1.0, 0.0).astype(bf16))
            ws.append(jnp.sum(jnp.where(one, wsel, 0.0), axis=1, keepdims=True))
            one = ranks == 32 + iota((16, ROWS), 0) % 4
            ohrs.append(jnp.where(one, 1.0, 0.0).astype(bf16))
            wrs.append(jnp.sum(jnp.where(one, wsel, 0.0), axis=1, keepdims=True))
        oh = jnp.concatenate(ohs + ohrs, axis=0)
        oh_ref[at(g * GO, GO, 16), :] = oh
        w = jnp.concatenate(ws + wrs, axis=0)
        def cut_tiles(t, j, store, members):
            ref = c_ref if t else x_ref
            main = dot(oh, ref[:, at(quarter(j) * QW, QW, QW)])
            if t:
                main = main * w
            rem = main[GM:]
            tail = jnp.zeros((GT, 128), f32)
            for cg in range(4):
                tail = jnp.where(tile_col == cg, rem[:, cg * 128 : (cg + 1) * 128], tail)
            main = main.astype(bf16)
            tail = tail.astype(bf16)
            for i in range(members):
                for rt in range(2):
                    for ct in range(4):
                        store(
                            i,
                            rt * 4 + ct,
                            main[
                                i * 32 + rt * 16 : i * 32 + rt * 16 + 16, ct * 128 : ct * 128 + 128
                            ],
                        )
                store(i, 8, tail[i * 16 : i * 16 + 16])

        def more(slot, members):
            for t in range(2):
                for j in range(2):

                    def store(i, tile, value):
                        more_ref[t, slot + i, j, tile] = value

                    cut_tiles(t, 2 + j, store, members)

        for t in range(2):
            for j in range(2):

                def store(i, tile, value):
                    send_ref[t, g * GB + i, j, tile] = value

                cut_tiles(t, j, store, GB)

        @pl.when(g == 0)
        def _():
            more(0, 2)

        @pl.when(g == 0)
        def _():
            pl.semaphore_wait(barrier, NSP - 1 + NTP - 1)
            for t in range(2):
                got_ref[t, 0, 0:2] = send_ref[t, 0]
                got_ref[t, 0, 2:4] = more_ref[t, 0]

        for t in range(2):
            for i in range(GB):
                k = g * GB + i

                @pl.when(k > 0)
                def _():
                    forward_copy(t, k, peer_at(k)).start()

                if i == 1:

                    @pl.when(g == 0)
                    def _():
                        more_copy(t, 1, k, peer_at(k)).start()

    ones = jnp.ones((8, FG), f32)
    spread = jnp.where(iota((8, 128), 0) == 0, 1.0, 0.0)
    spread1 = jnp.where(iota((8, 128), 0) == 1, 1.0, 0.0)

    def stat_copy(n, j):
        return remote(
            stat_ref.at[n, 0], stat_ref.at[n, NTP - j], ssend.at[n], srecv.at[n], me, quarter(j)
        )

    def stat_start(n, rows):
        stat_ref[n, 0] = rows
        for j in range(1, NTP):
            stat_copy(n, j).start()

    def stat_total(n):
        whole = stat_ref.at[n, pl.ds(1, NTP - 1)]
        remote(whole, whole, ssend.at[n], srecv.at[n], me, right).wait_recv()
        return (stat_ref[n, 0] + stat_ref[n, 1]) + (stat_ref[n, 2] + stat_ref[n, 3])

    def column(row_form, pick):
        one = exact_dot(row_form, pick, 0, 0)
        return jnp.concatenate([one, one], axis=1)


    def to_side(src, t, k, side):
        return remote(
            src,
            got_ref.at[t, k, 2 + side],
            xfsend.at[side],
            xfrecv.at[k // GB, side],
            me,
            to_left_or_right(side),
        )

    def pass_on(g):
        for t in range(2):

            @pl.loop(0, GB)
            def _(m):
                k = g * GB + m

                @pl.when(k > 0)
                def _():
                    forward_copy(t, k, source_at(k)).wait_recv()

                @pl.when(k > 1)
                def _():
                    to_side(got_ref.at[t, k, 0], t, k, 1).start()
                    to_side(got_ref.at[t, k, 1], t, k, 0).start()

    a = iota((GT, GT), 0)
    perm_col = (a % (GB * 4)) // 4 * 16 + (a // (GB * 4)) * 4 + a % 4
    perm = jnp.where(iota((GT, GT), 1) == perm_col, 1.0, 0.0).astype(bf16)

    def experts(g):
        base = g * GR
        first = g * GB
        def side_wait(start, size):
            for side in range(2):
                whole = got_ref.at[:, pl.ds(start, size), 2 + side]
                remote(
                    whole, whole, xfsend.at[side], xfrecv.at[g, side], me, to_left_or_right(side)
                ).wait_recv()

        @pl.when(g == 0)
        def _():
            side_wait(first + 2, GB - 2)

        @pl.when(g > 0)
        def _():
            side_wait(first, GB)

        @pl.when(g == 0)
        def _():
            for t in range(2):
                more_copy(t, 1, 1, source_at(1)).wait_recv()

        for t in range(2):
            for r in range(4):
                lane = quarter(r) * QW
                for i in range(GB):
                    for rt in range(2):
                        for ct in range(4):
                            rows_ref[
                                t,
                                at(base + i * 32 + rt * 16, 16, 16),
                                at(lane + ct * 128, 128, 128),
                            ] = got_ref[t, first + i, r, rt * 4 + ct]
                rem = dot(perm, got_ref[t, pl.ds(first, GB), r, 8].reshape(GT, 128)).astype(bf16)
                for cg in range(4):
                    rows_ref[
                        t, at(base + GM, GB * 4, 16), at(lane + cg * 128, 128, 128)
                    ] = rem[cg * GB * 4 : (cg + 1) * GB * 4]
        span = at(base, GR, 16)
        tok = rows_ref[0, span, :]
        pre_gate = dot(tok, wg_ref[...])
        pre_up = dot(tok, wu_ref[...])
        hidden_grad = dot(rows_ref[1, span, :], wd_ref[...], 1, 1)
        sig = jax.nn.sigmoid(pre_gate)
        act = pre_gate * sig
        hid_ref[0, span, :] = (act * pre_up).astype(bf16)
        gate_pre = (hidden_grad * pre_up * sig * (1.0 + pre_gate * (1.0 - sig))).astype(bf16)
        up_pre = (hidden_grad * act).astype(bf16)
        hid_ref[1, span, :] = gate_pre
        hid_ref[2, span, :] = up_pre
        for r in (2, 3, 0, 1):
            cols = at(quarter(r) * QW, QW, QW)
            part = dot(gate_pre, wg_ref[cols, :], 1, 1) + dot(up_pre, wu_ref[cols, :], 1, 1)
            part = part.astype(bf16)
            for i in range(GB):
                for rt in range(2):
                    for ct in range(4):
                        part_ref[r, first + i, rt * 4 + ct] = part[
                            i * 32 + rt * 16 : i * 32 + rt * 16 + 16, ct * 128 : ct * 128 + 128
                        ]
            stack = jnp.concatenate(
                [part[GM:GR, cg * 128 : cg * 128 + 128] for cg in range(4)], axis=0
            )
            rem = dot(perm, stack, 0, 0).astype(bf16)
            for i in range(GB):
                part_ref[r, first + i, 8] = rem[i * 16 : i * 16 + 16]
            if r >= 2:
                pair_copy(g, 3 - r).start()

    def pair_copy(g, side):
        group = pl.ds(g * GB, GB)
        return remote(
            part_ref.at[3 - side, group],
            pair_ref.at[side, group],
            xbsend.at[g, side],
            xbrecv.at[g, side],
            me,
            to_left_or_right(side),
        )

    def back_copy(g, m):
        k = g * GB + m
        return remote(
            back_ref.at[k], home_ref.at[k], bsend.at[g], brecv.at[g], source_at(k), x
        )

    def send_back(g):
        for side in range(2):
            pair_copy(g, side).wait_recv()

        @pl.loop(0, GB)
        def _(m):
            k = g * GB + m
            for j in range(2):
                both = part_ref[j, k].astype(f32) + pair_ref[j, k].astype(f32)
                back_ref[k, j] = both.astype(bf16)

            @pl.when(k > 0)
            def _():
                back_copy(g, m).start()

            @pl.when(k == 0)
            def _():
                home_ref[0] = back_ref[0]

    def home_wait(g):
        @pl.when(g == 0)
        def _():
            span = home_ref.at[pl.ds(1, GB - 1)]
            remote(span, span, bsend.at[g], brecv.at[g], peer_at(1), x).wait_recv()

        @pl.when(g > 0)
        def _():
            span = home_ref.at[pl.ds(g * GB, GB)]
            remote(span, span, bsend.at[g], brecv.at[g], peer_at(1), x).wait_recv()

    def combine(g, js=(0, 1)):
        oh = oh_ref[at(g * GO, GO, 16), :]
        for j in js:
            rows = []
            for i in range(GB):
                for rt in range(2):
                    rows.append(
                        jnp.concatenate(
                            [home_ref[g * GB + i, j, rt * 4 + ct] for ct in range(4)], axis=1
                        )
                    )
            rem = home_ref[pl.ds(g * GB, GB), j, 8].reshape(GT, 128).astype(f32)
            tails = [jnp.where(tile_col == cg, rem, 0.0).astype(bf16) for cg in range(4)]
            rows.append(jnp.concatenate(tails, axis=1))
            sum_ref[:, j * QW : (j + 1) * QW] += dot(oh, jnp.concatenate(rows, axis=0), 0, 0)

    sum_ref[...] = jnp.zeros_like(sum_ref)

    @pl.loop(0, NG)
    def _(g):
        prepare(g)

    @pl.loop(0, NG + 2)
    def _(step):
        @pl.when(step < NG)
        def _():
            pass_on(step)

        @pl.when(step == 0)
        def _():
            for load in loads[2:]:
                load.wait()
            stat_start(0, exact_dot(ones, co_ref[...].astype(f32), 1, 1))

        @pl.when((step > 0) & (step < NG + 1))
        def _():
            experts(step - 1)

        @pl.when(step > 1)
        def _():
            send_back(step - 2)

    def weight_grads(g):
        cols = pl.ds(g * QW, QW)
        tok = rows_ref[0, :, cols]
        gg_ref[cols, :] = dot(tok, hid_ref[1], 0, 0).astype(bf16)
        ug_ref[cols, :] = dot(tok, hid_ref[2], 0, 0).astype(bf16)
        dg_ref[:, cols] = dot(hid_ref[0], rows_ref[1, :, cols], 0, 0).astype(bf16)

    stores = [
        pltpu.make_async_copy(src, dst, outsem.at[n])
        for n, (src, dst) in enumerate(
            [(gg_ref, gg_hbm), (ug_ref, ug_hbm), (dg_ref, dg_hbm), (resid_ref, resid_hbm)]
        )
    ]
    weight_grads(0)

    conv = co_ref[...].astype(f32)
    mean = column(stat_total(0), spread) / CH
    centred = conv - mean
    stat_start(1, exact_dot(ones, centred * centred, 1, 1))
    var = column(stat_total(1), spread) / CH
    rstd = lax.rsqrt(var + norm_eps)
    normed = centred * rstd
    norm_pre = normed * gain_ref[...] + bias_ref[...]
    norm_sig = jax.nn.sigmoid(norm_pre)
    act_ref[...] = (norm_pre * norm_sig).astype(bf16)
    normed_ref[...] = normed
    rstd_ref[...] = rstd
    coef_ref[...] = norm_sig * (1.0 + norm_pre * (1.0 - norm_sig)) * gain_ref[...]

    @pl.loop(0, NG - 1)
    def _(g):
        home_wait(g)
        combine(g)

    home_wait(NG - 1)
    def exchange(side):
        return remote(
            exo_ref.at[side],
            exi_ref.at[side],
            esend.at[side],
            erecv.at[side],
            me,
            to_left_or_right(side),
        )

    combine(NG - 1, (1,))
    exo_ref[1] = sum_ref[:, QW : QW + 256].astype(bf16)
    exchange(1).start()
    combine(NG - 1, (0,))
    exo_ref[0] = sum_ref[:, 256:QW].astype(bf16)
    exchange(0).start()
    weight_grads(1)
    weight_grads(2)
    for side in range(2):
        exchange(side).wait_recv()
    cot0 = c_ref[:, at(quarter(0) * QW, 256, 256)].astype(f32)
    cot1 = c_ref[:, at(quarter(1) * QW + 256, 256, 256)].astype(f32)
    ag_ref[0, 0] = (cot0 + (sum_ref[:, :256] + exi_ref[1].astype(f32))).astype(bf16)
    ag_ref[0, 1] = (cot1 + (sum_ref[:, QW + 256 :] + exi_ref[0].astype(f32))).astype(bf16)

    def gather(side, part):
        return remote(
            ag_ref.at[0, part],
            ag_ref.at[3 if side else 1, part],
            asend.at[side, part],
            arecv.at[side, part],
            me,
            to_left_or_right(side),
        )

    def gather_far(side):
        return remote(
            ag_ref.at[3 if side else 1, 1 - side],
            ag_ref.at[2, 1 - side],
            asend.at[2, side],
            arecv.at[2, side],
            me,
            to_left_or_right(side),
        )

    def place(o, part):
        cols = at(quarter(o + part) * QW + part * 256, 256, 256)
        resid_ref[:, cols] = ag_ref[o, part]
        return dot(ag_ref[o, part], ow_ref[:, cols], 1, 1)

    def owg_copy(peer):
        return remote(pso_ref.at[peer], psi_ref.at[me], psend.at[0], precv.at[0], peer, x)

    def project(o, part):
        term = dot(ag_ref[o, part], act_ref[...], 0, 0).astype(bf16)
        for i in range(4):
            peer = quarter(o + part) * 8 + part * 4 + i
            for rt in range(4):
                for ct in range(2):
                    pso_ref[peer, rt * 2 + ct] = term[
                        i * OW + rt * 16 : i * OW + rt * 16 + 16, ct * 128 : ct * 128 + 128
                    ]

        for i in range(4):
            peer = quarter(o + part) * 8 + part * 4 + (i + me) % 4

            @pl.when(peer == me)
            def _():
                psi_ref[me] = pso_ref[me]

            @pl.when(peer != me)
            def _():
                owg_copy(peer).start()

    for side in range(2):
        gather(side, 1 - side).start()
    for side in range(2):
        gather(side, side).start()
    mix_grad = place(0, 0) + place(0, 1)
    project(0, 0)
    project(0, 1)
    weight_grads(3)
    for store in stores[:3]:
        store.start()
    for side in range(2):
        gather(side, 1 - side).wait_recv()
        gather_far(side).start()
    mix_grad = mix_grad + place(1, 1) + place(3, 0)
    project(1, 1)
    project(3, 0)
    for side in range(2):
        gather(side, side).wait_recv()
    mix_grad = mix_grad + place(1, 0) + place(3, 1)
    project(1, 0)
    project(3, 1)
    for side in range(2):
        gather_far(side).wait_recv()
    mix_grad = mix_grad + place(2, 0) + place(2, 1)
    stores[3].start()

    norm_grad = mix_grad * coef_ref[...]
    sum_rows = exact_dot(ones, norm_grad, 1, 1)
    dot_rows = exact_dot(ones, norm_grad * normed_ref[...], 1, 1)
    stat_start(2, jnp.where(iota((8, ROWS), 0) == 0, sum_rows, dot_rows))

    project(2, 0)
    project(2, 1)
    totals = stat_total(2)
    conv_grad = rstd_ref[...] * (
        norm_grad
        - column(totals, spread) / CH
        - normed_ref[...] * (column(totals, spread1) / CH)
    )
    ext_ref[0:ROWS, :] = conv_grad

    def halo_copy(sp):
        return remote(ext_ref.at[0:32], halo_ref, hsend.at[0], hrecv.at[0], sp, x)

    @pl.when(me > 0)
    def _():
        halo_copy(me - 1).start()

    def convolve(start, rows):
        glu = jnp.zeros((rows, FG), f32)
        for lag in range(KW):
            begin = start + KW - 1 - lag
            glu = glu + taps_ref[lag : lag + 1, :] * ext_ref[begin : begin + rows, :]
        span = pl.ds(start, rows)
        gate_sig = jax.nn.sigmoid(cg_ref[span, :].astype(f32))
        value_ref[span, :] = (glu * gate_sig).astype(bf16)
        gatein_ref[span, :] = (
            glu * cv_ref[span, :].astype(f32) * gate_sig * (1.0 - gate_sig)
        ).astype(bf16)

    for start in range(0, ROWS - 32, 32):
        convolve(start, 32)

    @pl.when(me < NSP - 1)
    def _():
        halo_copy(me + 1).wait_recv()
        ext_ref[ROWS : ROWS + 32, :] = halo_ref[...]

    @pl.when(me == NSP - 1)
    def _():
        ext_ref[ROWS : ROWS + 32, :] = jnp.zeros((32, FG), f32)

    convolve(ROWS - 32, 32)

    whole = psi_ref.at[pl.ds(0, NSP - 1)]
    remote(whole, whole, psend.at[0], precv.at[0], me, right).wait_recv()
    for rt in range(4):
        for ct in range(2):
            total = psi_ref[0, rt * 2 + ct].astype(f32)
            for k in range(1, NSP):
                total = total + psi_ref[k, rt * 2 + ct].astype(f32)
            owg_ref[rt * 16 : rt * 16 + 16, ct * 128 : ct * 128 + 128] = total

    @pl.when(me > 0)
    def _():
        halo_copy(me - 1).wait_send()

    remote(whole, whole, psend.at[0], precv.at[0], me, right).wait_send()
    for n in range(3):
        sent = stat_ref.at[n, pl.ds(1, NTP - 1)]
        remote(sent, sent, ssend.at[n], srecv.at[n], me, right).wait_send()
    for side in range(2):
        exchange(side).wait_send()
        gather(side, 0).wait_send()
        gather(side, 1).wait_send()
        gather_far(side).wait_send()
        sent = got_ref.at[:, pl.ds(0, NSP - WHOLE), side]
        remote(sent, sent, xfsend.at[side], xfrecv.at[0, side], me, right).wait_send()
        for g in range(NG):
            pair_copy(g, side).wait_send()
    for t in range(2):
        sent = send_ref.at[t, pl.ds(0, NSP - 1)]
        remote(sent, sent, fsend.at[t], frecv.at[t, 0], me, right).wait_send()
    sent = more_ref.at[:, pl.ds(0, WHOLE - 1)]
    remote(sent, sent, msend.at[0], mrecv.at[0, 0], me, right).wait_send()
    for g in range(NG):
        sent = back_ref.at[pl.ds(0, GB - 1 if g == 0 else GB)]
        remote(sent, sent, bsend.at[g], brecv.at[g], me, right).wait_send()
    for store in stores:
        store.wait()


def widen_kernel(*refs):
    half = len(refs) // 2
    for src, dst in zip(refs[:half], refs[half:]):
        dst[...] = src[...].astype(dst.dtype)


def on_device(
    expert_input,
    cotangent,
    routes,
    route_weight,
    expert_gate,
    expert_up,
    expert_down,
    conv_out,
    conv_value,
    conv_gate,
    conv_taps,
    norm_gain,
    norm_bias,
    out_weight,
):
    dma = pltpu.SemaphoreType.DMA
    vmem = pl.BlockSpec(memory_space=pltpu.VMEM)
    anywhere = pl.BlockSpec(memory_space=pl.ANY)
    shape = jax.ShapeDtypeStruct
    gate_grad, up_grad, down_grad, resid_grad, projected, value_grad, gate_in_grad = pl.pallas_call(
        layer_kernel,
        out_shape=(
            shape((D, FG), bf16),
            shape((D, FG), bf16),
            shape((FG, D), bf16),
            shape((ROWS, D), bf16),
            shape((OW, FG), f32),
            shape((ROWS, FG), bf16),
            shape((ROWS, FG), bf16),
        ),
        in_specs=[anywhere] * 9 + [vmem] * 5,
        out_specs=(anywhere,) * 4 + (vmem,) * 3,
        scratch_shapes=[
            pltpu.VMEM((ROWS, D), bf16),
            pltpu.VMEM((ROWS, D), bf16),
            pltpu.VMEM((D, FG), bf16),
            pltpu.VMEM((D, FG), bf16),
            pltpu.VMEM((FG, D), bf16),
            pltpu.VMEM((FG, D), bf16),
            pltpu.VMEM((ROWS, FG), bf16),
            pltpu.VMEM((ROWS, FG), bf16),
            pltpu.VMEM((ROWS, FG), bf16),
            pltpu.VMEM((D, FG), bf16),
            pltpu.VMEM((D, FG), bf16),
            pltpu.VMEM((FG, D), bf16),
            pltpu.VMEM((ROWS, D), bf16),
            pltpu.VMEM((NSP, ROWS), jnp.int32),
            pltpu.VMEM((NSP, ROWS), f32),
            pltpu.VMEM((NG * GO, ROWS), bf16),
            pltpu.VMEM((2, NSP, 2, NT, 16, 128), bf16),
            pltpu.VMEM((2, WHOLE, 2, NT, 16, 128), bf16),
            pltpu.VMEM((2, NSP, 4, NT, 16, 128), bf16),
            pltpu.VMEM((2, NSP * 36, D), bf16),
            pltpu.VMEM((3, NSP * 36, FG), bf16),
            pltpu.VMEM((4, NSP, NT, 16, 128), bf16),
            pltpu.VMEM((2, NSP, NT, 16, 128), bf16),
            pltpu.VMEM((NSP, 2, NT, 16, 128), bf16),
            pltpu.VMEM((NSP, 2, NT, 16, 128), bf16),
            pltpu.VMEM((ROWS, 2 * QW), f32),
            pltpu.VMEM((2, ROWS, 256), bf16),
            pltpu.VMEM((2, ROWS, 256), bf16),
            pltpu.VMEM((4, 2, ROWS, 256), bf16),
            pltpu.VMEM((3, NTP, 8, ROWS), f32),
            pltpu.VMEM((ROWS, FG), f32),
            pltpu.VMEM((ROWS, FG), f32),
            pltpu.VMEM((ROWS, FG), f32),
            pltpu.VMEM((ROWS, FG), bf16),
            pltpu.VMEM((ROWS + 32, FG), f32),
            pltpu.VMEM((32, FG), f32),
            pltpu.VMEM((NSP, 8, 16, 128), bf16),
            pltpu.VMEM((NSP, 8, 16, 128), bf16),
            dma((9,)),
            dma((4,)),
            dma((2,)),
            dma((2, NSP)),
            dma((1,)),
            dma((2, WHOLE)),
            dma((2,)),
            dma((NG, 2)),
            dma((NG, 2)),
            dma((NG, 2)),
            dma((NG,)),
            dma((NG,)),
            dma((2,)),
            dma((2,)),
            dma((3, 2)),
            dma((3, 2)),
            dma((3,)),
            dma((3,)),
            dma((1,)),
            dma((1,)),
            dma((1,)),
            dma((1,)),
        ],
        compiler_params=pltpu.CompilerParams(
            collective_id=0, has_side_effects=True, vmem_limit_bytes=67000000
        ),
        name="layer",
    )(
        expert_input,
        cotangent,
        expert_gate[0],
        expert_up[0],
        expert_down[0],
        out_weight,
        conv_out,
        conv_value,
        conv_gate,
        routes.T,
        route_weight.T,
        conv_taps,
        norm_gain[None, :],
        norm_bias[None, :],
    )
    steps = 4

    def block(rows, cols):
        return pl.BlockSpec((rows // steps, cols), lambda n: (n, 0))

    sizes = [(D, FG), (D, FG), (FG, D), (ROWS, D), (OW, FG), (ROWS, FG), (ROWS, FG)]
    types = [f32, f32, f32, bf16, f32, bf16, bf16]
    gate_grad, up_grad, down_grad, resid_grad, projected, value_grad, gate_in_grad = pl.pallas_call(
        widen_kernel,
        grid=(steps,),
        out_shape=tuple(shape(size, kind) for size, kind in zip(sizes, types)),
        in_specs=[block(*size) for size in sizes],
        out_specs=tuple(block(*size) for size in sizes),
        name="widen",
    )(gate_grad, up_grad, down_grad, resid_grad, projected, value_grad, gate_in_grad)
    return (
        gate_grad[None],
        up_grad[None],
        down_grad[None],
        resid_grad,
        projected.T,
        value_grad,
        gate_in_grad,
    )


def solution(mesh):
    return jax.shard_map(
        on_device,
        mesh=mesh,
        in_specs=(
            P("sp", None),
            P("sp", None),
            P("sp", None),
            P("sp", None),
            P("sp", None, "tp"),
            P("sp", None, "tp"),
            P("sp", "tp", None),
            P("sp", "tp"),
            P("sp", "tp"),
            P("sp", "tp"),
            P(None, "tp"),
            P("tp"),
            P("tp"),
            P("tp", None),
        ),
        out_specs=(
            P("sp", None, "tp"),
            P("sp", None, "tp"),
            P("sp", "tp", None),
            P("sp", None),
            P("tp", "sp"),
            P("sp", "tp"),
            P("sp", "tp"),
        ),
        check_vma=False,
    )
```

```python
import jax
import jax.numpy as jnp
from jax import lax
from jax.experimental import pallas as pl
from jax.experimental.pallas import tpu as pltpu
from jax.sharding import PartitionSpec as P

MESH = pl.DeviceIdType.MESH
bf16 = jnp.bfloat16
f32 = jnp.float32
norm_eps = 1e-06

NSP = 32
NTP = 4
ROWS = 384
D = 2048
CH = 1024
KW = 31
QW = 512
FG = 256
NG = 8
GB = NSP // NG
GR = GB * 36
GM = GB * 32
GT = GB * 16
GO = GM + GT
NT = 9
WHOLE = 2
OW = D // NSP


def dot(a, b, ca=1, cb=0, precision=None):
    return lax.dot_general(
        a, b, (((ca,), (cb,)), ((), ())), preferred_element_type=f32, precision=precision
    )


def exact_dot(a, b, ca=1, cb=0):
    return dot(a, b, ca, cb, lax.Precision.HIGHEST)


def split(a):
    high = a.astype(bf16)
    return high, (a - high.astype(f32)).astype(bf16)


def row_sums(a):
    high, low = split(a)
    return dot(jnp.ones((8, 2 * FG), bf16), jnp.concatenate([high, low], axis=1), 1, 1)


def iota(shape, dim):
    return lax.broadcasted_iota(jnp.int32, shape, dim)


def at(start, size, step):
    return pl.ds(pl.multiple_of(start, step), size)


def layer_kernel(
    x_hbm,
    c_hbm,
    wg_hbm,
    wu_hbm,
    wd_hbm,
    ow_hbm,
    co_hbm,
    cv_hbm,
    cg_hbm,
    routes_ref,
    weight_ref,
    taps_ref,
    gain_ref,
    bias_ref,
    gg_hbm,
    ug_hbm,
    dg_hbm,
    resid_hbm,
    owg_ref,
    value_ref,
    gatein_ref,
    x_ref,
    c_ref,
    wg_ref,
    wu_ref,
    wd_ref,
    ow_ref,
    co_ref,
    cv_ref,
    cg_ref,
    gg_ref,
    ug_ref,
    dg_ref,
    resid_ref,
    rank_ref,
    wsel_ref,
    oh_ref,
    send_ref,
    more_ref,
    got_ref,
    rows_ref,
    hid_ref,
    part_ref,
    pair_ref,
    back_ref,
    home_ref,
    sum_ref,
    exo_ref,
    exi_ref,
    ag_ref,
    stat_ref,
    normed_ref,
    coef_ref,
    rstd_ref,
    act_ref,
    ext_ref,
    halo_ref,
    pso_ref,
    psi_ref,
    pin_ref,
    insem,
    outsem,
    fsend,
    frecv,
    msend,
    mrecv,
    xfsend,
    xfrecv,
    xbsend,
    xbrecv,
    bsend,
    brecv,
    esend,
    erecv,
    asend,
    arecv,
    ssend,
    srecv,
    hsend,
    hrecv,
    psend,
    precv,
    dsend,
    drecv,
):
    me = lax.axis_index("sp")
    x = lax.axis_index("tp")
    z, y, core = me // 8, (me // 2) % 4, me % 2
    right, left = (x + 1) % NTP, (x + 3) % NTP

    def offset(k):
        g, m = k // GB, k % GB
        lap, part = g * 4 // NG, g % (NG // 4)
        dz = part + (m // 2) * (NG // 4)
        return dz, (dz + lap) % 4, m % 2

    def peer_at(k):
        dz, dy, dc = offset(k)
        return ((z + dz) % 4) * 8 + ((y + dy) % 4) * 2 + (core + dc) % 2

    def source_at(k):
        dz, dy, dc = offset(k)
        return ((z + 4 - dz) % 4) * 8 + ((y + 4 - dy) % 4) * 2 + (core + dc) % 2

    def quarter(j):
        return (x + j) % NTP

    def remote(src, dst, send, recv, sp, tp):
        return pltpu.make_async_remote_copy(
            src_ref=src,
            dst_ref=dst,
            send_sem=send,
            recv_sem=recv,
            device_id=(sp, tp),
            device_id_type=MESH,
        )

    def to_left_or_right(side):
        return right if side else left

    loads = [
        pltpu.make_async_copy(src, dst, insem.at[n])
        for n, (src, dst) in enumerate(
            [
                (x_hbm, x_ref),
                (c_hbm, c_ref),
                (wg_hbm, wg_ref),
                (wu_hbm, wu_ref),
                (wd_hbm, wd_ref),
                (co_hbm, co_ref),
                (ow_hbm, ow_ref),
                (cv_hbm, cv_ref),
                (cg_hbm, cg_ref),
            ]
        )
    ]
    for load in loads:
        load.start()

    barrier = pltpu.get_barrier_semaphore()

    @pl.loop(1, NSP)
    def _(k):
        pl.semaphore_signal(barrier, inc=1, device_id=(peer_at(k), x), device_id_type=MESH)

    for j in range(1, NTP):
        pl.semaphore_signal(barrier, inc=1, device_id=(me, quarter(j)), device_id_type=MESH)

    r0, r1 = routes_ref[0:1, :], routes_ref[1:2, :]
    names = iota((NSP, ROWS), 0)
    m0, m1 = r0 == names, r1 == names
    member = jnp.where(m0 | m1, 1.0, 0.0).astype(bf16)
    before = jnp.where(iota((ROWS, ROWS), 0) < iota((ROWS, ROWS), 1), 1.0, 0.0).astype(bf16)
    rank = dot(member, before)
    rank_ref[...] = jnp.where(m0 | m1, rank, -1.0).astype(jnp.int32)
    wsel_ref[...] = jnp.where(m0, weight_ref[0:1, :], jnp.where(m1, weight_ref[1:2, :], 0.0))
    loads[0].wait()
    loads[1].wait()

    def forward_copy(t, k, peer):
        return remote(
            send_ref.at[t, k], got_ref.at[t, k, 0:2], fsend.at[t], frecv.at[t, k], peer, x
        )

    def more_copy(t, slot, k, peer):
        return remote(
            more_ref.at[t, slot], got_ref.at[t, k, 2:4], msend.at[0], mrecv.at[t, slot], peer, x
        )

    tile_col = (iota((GT, 128), 0) % 16) // 4

    def prepare(g):
        ohs, ws, ohrs, wrs = [], [], [], []
        for i in range(GB):
            peer = peer_at(g * GB + i)
            ranks = rank_ref[pl.ds(peer, 1), :]
            wsel = wsel_ref[pl.ds(peer, 1), :]
            one = ranks == iota((32, ROWS), 0)
            ohs.append(jnp.where(one, 1.0, 0.0).astype(bf16))
            ws.append(jnp.sum(jnp.where(one, wsel, 0.0), axis=1, keepdims=True))
            one = ranks == 32 + iota((16, ROWS), 0) % 4
            ohrs.append(jnp.where(one, 1.0, 0.0).astype(bf16))
            wrs.append(jnp.sum(jnp.where(one, wsel, 0.0), axis=1, keepdims=True))
        oh = jnp.concatenate(ohs + ohrs, axis=0)
        oh_ref[at(g * GO, GO, 16), :] = oh
        w = jnp.concatenate(ws + wrs, axis=0)
        def cut_tiles(t, j, store, members):
            ref = c_ref if t else x_ref
            main = dot(oh, ref[:, at(quarter(j) * QW, QW, QW)])
            if t:
                main = main * w
            rem = main[GM:]
            tail = jnp.zeros((GT, 128), f32)
            for cg in range(4):
                tail = jnp.where(tile_col == cg, rem[:, cg * 128 : (cg + 1) * 128], tail)
            main = main.astype(bf16)
            tail = tail.astype(bf16)
            for i in range(members):
                for rt in range(2):
                    for ct in range(4):
                        store(
                            i,
                            rt * 4 + ct,
                            main[
                                i * 32 + rt * 16 : i * 32 + rt * 16 + 16, ct * 128 : ct * 128 + 128
                            ],
                        )
                store(i, 8, tail[i * 16 : i * 16 + 16])

        def more(slot, members):
            for t in range(2):
                for j in range(2):

                    def store(i, tile, value):
                        more_ref[t, slot + i, j, tile] = value

                    cut_tiles(t, 2 + j, store, members)

        for t in range(2):
            for j in range(2):

                def store(i, tile, value):
                    send_ref[t, g * GB + i, j, tile] = value

                cut_tiles(t, j, store, GB)

        @pl.when(g == 0)
        def _():
            more(0, 2)

        @pl.when(g == 0)
        def _():
            pl.semaphore_wait(barrier, NSP - 1 + NTP - 1)
            for t in range(2):
                got_ref[t, 0, 0:2] = send_ref[t, 0]
                got_ref[t, 0, 2:4] = more_ref[t, 0]

        for t in range(2):
            for i in range(GB):
                k = g * GB + i

                @pl.when(k > 0)
                def _():
                    forward_copy(t, k, peer_at(k)).start()

                if i == 1:

                    @pl.when(g == 0)
                    def _():
                        more_copy(t, 1, k, peer_at(k)).start()

    ones = jnp.ones((8, FG), f32)
    spread = jnp.where(iota((8, 128), 0) == 0, 1.0, 0.0)
    spread1 = jnp.where(iota((8, 128), 0) == 1, 1.0, 0.0)

    def stat_copy(n, j):
        return remote(
            stat_ref.at[n, 0], stat_ref.at[n, NTP - j], ssend.at[n], srecv.at[n], me, quarter(j)
        )

    def stat_start(n, rows):
        stat_ref[n, 0] = rows
        for j in range(1, NTP):
            stat_copy(n, j).start()

    def stat_total(n):
        whole = stat_ref.at[n, pl.ds(1, NTP - 1)]
        remote(whole, whole, ssend.at[n], srecv.at[n], me, right).wait_recv()
        return (stat_ref[n, 0] + stat_ref[n, 1]) + (stat_ref[n, 2] + stat_ref[n, 3])

    def column(row_form, pick):
        high, low = split(row_form)
        low2 = (row_form - high.astype(f32) - low.astype(f32)).astype(bf16)
        terms = jnp.concatenate([high, low, low2, jnp.zeros_like(high)], axis=0)
        one = dot(terms, jnp.concatenate([pick] * 4, axis=0).astype(bf16), 0, 0)
        return jnp.concatenate([one, one], axis=1)


    def to_side(src, t, k, side):
        return remote(
            src,
            got_ref.at[t, k, 2 + side],
            xfsend.at[side],
            xfrecv.at[k // GB, side],
            me,
            to_left_or_right(side),
        )

    def pass_on(g):
        for t in range(2):

            @pl.loop(0, GB)
            def _(m):
                k = g * GB + m

                @pl.when(k > 0)
                def _():
                    forward_copy(t, k, source_at(k)).wait_recv()

                @pl.when(k > 1)
                def _():
                    to_side(got_ref.at[t, k, 0], t, k, 1).start()
                    to_side(got_ref.at[t, k, 1], t, k, 0).start()

    a = iota((GT, GT), 0)
    perm_col = (a % (GB * 4)) // 4 * 16 + (a // (GB * 4)) * 4 + a % 4
    perm = jnp.where(iota((GT, GT), 1) == perm_col, 1.0, 0.0).astype(bf16)

    def experts(g):
        base = g * GR
        first = g * GB
        def side_wait(start, size):
            for side in range(2):
                whole = got_ref.at[:, pl.ds(start, size), 2 + side]
                remote(
                    whole, whole, xfsend.at[side], xfrecv.at[g, side], me, to_left_or_right(side)
                ).wait_recv()

        @pl.when(g == 0)
        def _():
            side_wait(first + 2, GB - 2)

        @pl.when(g > 0)
        def _():
            side_wait(first, GB)

        @pl.when(g == 0)
        def _():
            for t in range(2):
                more_copy(t, 1, 1, source_at(1)).wait_recv()

        for t in range(2):
            for r in range(4):
                lane = quarter(r) * QW
                for i in range(GB):
                    for rt in range(2):
                        for ct in range(4):
                            rows_ref[
                                t,
                                at(base + i * 32 + rt * 16, 16, 16),
                                at(lane + ct * 128, 128, 128),
                            ] = got_ref[t, first + i, r, rt * 4 + ct]
                rem = dot(perm, got_ref[t, pl.ds(first, GB), r, 8].reshape(GT, 128)).astype(bf16)
                for cg in range(4):
                    rows_ref[
                        t, at(base + GM, GB * 4, 16), at(lane + cg * 128, 128, 128)
                    ] = rem[cg * GB * 4 : (cg + 1) * GB * 4]
        span = at(base, GR, 16)
        tok = rows_ref[0, span, :]
        pre_gate = dot(tok, wg_ref[...])
        pre_up = dot(tok, wu_ref[...])
        hidden_grad = dot(rows_ref[1, span, :], wd_ref[...], 1, 1)
        sig = jax.nn.sigmoid(pre_gate)
        act = pre_gate * sig
        hid_ref[0, span, :] = (act * pre_up).astype(bf16)
        gate_pre = (hidden_grad * pre_up * sig * (1.0 + pre_gate * (1.0 - sig))).astype(bf16)
        up_pre = (hidden_grad * act).astype(bf16)
        hid_ref[1, span, :] = gate_pre
        hid_ref[2, span, :] = up_pre
        for r in (2, 3, 0, 1):
            cols = at(quarter(r) * QW, QW, QW)
            part = dot(gate_pre, wg_ref[cols, :], 1, 1) + dot(up_pre, wu_ref[cols, :], 1, 1)
            part = part.astype(bf16)
            for i in range(GB):
                for rt in range(2):
                    for ct in range(4):
                        part_ref[r, first + i, rt * 4 + ct] = part[
                            i * 32 + rt * 16 : i * 32 + rt * 16 + 16, ct * 128 : ct * 128 + 128
                        ]
            stack = jnp.concatenate(
                [part[GM:GR, cg * 128 : cg * 128 + 128] for cg in range(4)], axis=0
            )
            rem = dot(perm, stack, 0, 0).astype(bf16)
            for i in range(GB):
                part_ref[r, first + i, 8] = rem[i * 16 : i * 16 + 16]
            if r >= 2:
                pair_copy(g, 3 - r).start()

    def pair_copy(g, side):
        group = pl.ds(g * GB, GB)
        return remote(
            part_ref.at[3 - side, group],
            pair_ref.at[side, group],
            xbsend.at[g, side],
            xbrecv.at[g, side],
            me,
            to_left_or_right(side),
        )

    def back_copy(g, m):
        k = g * GB + m
        return remote(
            back_ref.at[k], home_ref.at[k], bsend.at[g], brecv.at[g], source_at(k), x
        )

    def send_back(g):
        for side in range(2):
            pair_copy(g, side).wait_recv()

        @pl.loop(0, GB)
        def _(m):
            k = g * GB + m
            for j in range(2):
                both = part_ref[j, k].astype(f32) + pair_ref[j, k].astype(f32)
                back_ref[k, j] = both.astype(bf16)

            @pl.when(k > 0)
            def _():
                back_copy(g, m).start()

            @pl.when(k == 0)
            def _():
                home_ref[0] = back_ref[0]

    def home_wait(g):
        @pl.when(g == 0)
        def _():
            span = home_ref.at[pl.ds(1, GB - 1)]
            remote(span, span, bsend.at[g], brecv.at[g], peer_at(1), x).wait_recv()

        @pl.when(g > 0)
        def _():
            span = home_ref.at[pl.ds(g * GB, GB)]
            remote(span, span, bsend.at[g], brecv.at[g], peer_at(1), x).wait_recv()

    def combine(g, js=(0, 1)):
        oh = oh_ref[at(g * GO, GO, 16), :]
        for j in js:
            rows = []
            for i in range(GB):
                for rt in range(2):
                    rows.append(
                        jnp.concatenate(
                            [home_ref[g * GB + i, j, rt * 4 + ct] for ct in range(4)], axis=1
                        )
                    )
            rem = home_ref[pl.ds(g * GB, GB), j, 8].reshape(GT, 128).astype(f32)
            tails = [jnp.where(tile_col == cg, rem, 0.0).astype(bf16) for cg in range(4)]
            rows.append(jnp.concatenate(tails, axis=1))
            sum_ref[:, j * QW : (j + 1) * QW] += dot(oh, jnp.concatenate(rows, axis=0), 0, 0)

    sum_ref[...] = jnp.zeros_like(sum_ref)

    @pl.loop(0, NG)
    def _(g):
        prepare(g)

    @pl.loop(0, NG + 2)
    def _(step):
        @pl.when(step < NG)
        def _():
            pass_on(step)

        @pl.when(step == 0)
        def _():
            for load in loads[2:]:
                load.wait()
            stat_start(0, exact_dot(ones, co_ref[...].astype(f32), 1, 1))

        @pl.when(step == 2)
        def _():
            mean = column(stat_total(0), spread) / CH
            centred = co_ref[...].astype(f32) - mean
            normed_ref[...] = centred
            stat_start(1, exact_dot(ones, centred * centred, 1, 1))

        @pl.when(step == 4)
        def _():
            var = column(stat_total(1), spread) / CH
            rstd = lax.rsqrt(var + norm_eps)
            normed = normed_ref[...] * rstd
            norm_pre = normed * gain_ref[...] + bias_ref[...]
            norm_sig = jax.nn.sigmoid(norm_pre)
            act_ref[...] = (norm_pre * norm_sig).astype(bf16)
            normed_ref[...] = normed
            rstd_ref[...] = rstd
            coef_ref[...] = norm_sig * (1.0 + norm_pre * (1.0 - norm_sig)) * gain_ref[...]

        @pl.when((step > 0) & (step < NG + 1))
        def _():
            experts(step - 1)

        @pl.when(step > 1)
        def _():
            send_back(step - 2)

    def weight_grads(g):
        cols = pl.ds(g * QW, QW)
        tok = rows_ref[0, :, cols]
        gg_ref[cols, :] = dot(tok, hid_ref[1], 0, 0).astype(bf16)
        ug_ref[cols, :] = dot(tok, hid_ref[2], 0, 0).astype(bf16)
        dg_ref[:, cols] = dot(hid_ref[0], rows_ref[1, :, cols], 0, 0).astype(bf16)

    stores = [
        pltpu.make_async_copy(src, dst, outsem.at[n])
        for n, (src, dst) in enumerate(
            [(gg_ref, gg_hbm), (ug_ref, ug_hbm), (dg_ref, dg_hbm), (resid_ref, resid_hbm)]
        )
    ]
    weight_grads(0)

    @pl.loop(0, NG - 1)
    def _(g):
        home_wait(g)
        combine(g)

    home_wait(NG - 1)
    def exchange(side):
        return remote(
            exo_ref.at[side],
            exi_ref.at[side],
            esend.at[side],
            erecv.at[side],
            me,
            to_left_or_right(side),
        )

    combine(NG - 1, (1,))
    exo_ref[1] = sum_ref[:, QW : QW + 256].astype(bf16)
    exchange(1).start()
    combine(NG - 1, (0,))
    exo_ref[0] = sum_ref[:, 256:QW].astype(bf16)
    exchange(0).start()
    weight_grads(1)
    weight_grads(2)
    for side in range(2):
        exchange(side).wait_recv()
    cot0 = c_ref[:, at(quarter(0) * QW, 256, 256)].astype(f32)
    cot1 = c_ref[:, at(quarter(1) * QW + 256, 256, 256)].astype(f32)
    ag_ref[0, 0] = (cot0 + (sum_ref[:, :256] + exi_ref[1].astype(f32))).astype(bf16)
    ag_ref[0, 1] = (cot1 + (sum_ref[:, QW + 256 :] + exi_ref[0].astype(f32))).astype(bf16)

    def gather(side, part):
        return remote(
            ag_ref.at[0, part],
            ag_ref.at[3 if side else 1, part],
            asend.at[side, part],
            arecv.at[side, part],
            me,
            to_left_or_right(side),
        )

    def gather_far(side):
        return remote(
            ag_ref.at[3 if side else 1, 1 - side],
            ag_ref.at[2, 1 - side],
            asend.at[2, side],
            arecv.at[2, side],
            me,
            to_left_or_right(side),
        )

    def place(o, part):
        cols = at(quarter(o + part) * QW + part * 256, 256, 256)
        resid_ref[:, cols] = ag_ref[o, part]
        return dot(ag_ref[o, part], ow_ref[:, cols], 1, 1)

    def owner(o, part, i):
        return quarter(o + part) * 8 + part * 4 + i

    def partner_copy(o, peer):
        return remote(
            pso_ref.at[peer],
            pin_ref.at[peer // 2],
            dsend.at[0],
            drecv.at[o],
            (me // 2) * 2 + 1 - core,
            x,
        )

    def owg_copy(peer):
        return remote(
            pso_ref.at[peer], psi_ref.at[me // 2], psend.at[0], precv.at[0], peer, x
        )

    def project(o, part):
        term = dot(ag_ref[o, part], act_ref[...], 0, 0).astype(bf16)
        for i in range(4):
            for rt in range(4):
                for ct in range(2):
                    pso_ref[owner(o, part, i), rt * 2 + ct] = term[
                        i * OW + rt * 16 : i * OW + rt * 16 + 16, ct * 128 : ct * 128 + 128
                    ]
        for i in range(2):
            partner_copy(o, owner(o, part, 2 * i + 1 - core)).start()

    def relay(o):
        four = pin_ref.at[pl.ds(0, 4)]
        remote(four, four, dsend.at[0], drecv.at[o], me, right).wait_recv()
        for part in range(2):
            for i in range(2):
                peer = owner(o, part, 2 * i + core)
                both = pso_ref[peer].astype(f32) + pin_ref[peer // 2].astype(f32)
                pso_ref[peer] = both.astype(bf16)

                @pl.when(peer == me)
                def _():
                    psi_ref[me // 2] = pso_ref[me]

                @pl.when(peer != me)
                def _():
                    owg_copy(peer).start()

    for side in range(2):
        gather(side, 1 - side).start()
    for side in range(2):
        gather(side, side).start()
    mix_grad = place(0, 0) + place(0, 1)
    project(0, 0)
    project(0, 1)
    weight_grads(3)
    for store in stores[:3]:
        store.start()
    for side in range(2):
        gather(side, 1 - side).wait_recv()
        gather_far(side).start()
    mix_grad = mix_grad + place(1, 1) + place(3, 0)
    relay(0)
    project(1, 1)
    project(3, 0)
    for side in range(2):
        gather(side, side).wait_recv()
    mix_grad = mix_grad + place(1, 0) + place(3, 1)
    project(1, 0)
    project(3, 1)
    relay(1)
    relay(3)
    for side in range(2):
        gather_far(side).wait_recv()
    mix_grad = mix_grad + place(2, 0) + place(2, 1)
    stores[3].start()

    norm_grad = mix_grad * coef_ref[...]
    sum_rows = row_sums(norm_grad)
    dot_rows = row_sums(norm_grad * normed_ref[...])
    stat_start(2, jnp.where(iota((8, ROWS), 0) == 0, sum_rows, dot_rows))

    project(2, 0)
    project(2, 1)
    relay(2)
    totals = stat_total(2)
    conv_grad = rstd_ref[...] * (
        norm_grad
        - column(totals, spread) / CH
        - normed_ref[...] * (column(totals, spread1) / CH)
    )
    ext_ref[0:ROWS, :] = conv_grad

    def halo_copy(sp):
        return remote(ext_ref.at[0:32], halo_ref, hsend.at[0], hrecv.at[0], sp, x)

    @pl.when(me > 0)
    def _():
        halo_copy(me - 1).start()

    def convolve(start, rows):
        glu = jnp.zeros((rows, FG), f32)
        for lag in range(KW):
            begin = start + KW - 1 - lag
            glu = glu + taps_ref[lag : lag + 1, :] * ext_ref[begin : begin + rows, :]
        span = pl.ds(start, rows)
        gate_sig = jax.nn.sigmoid(cg_ref[span, :].astype(f32))
        value_ref[span, :] = (glu * gate_sig).astype(bf16)
        gatein_ref[span, :] = (
            glu * cv_ref[span, :].astype(f32) * gate_sig * (1.0 - gate_sig)
        ).astype(bf16)

    for start in range(0, ROWS - 32, 32):
        convolve(start, 32)

    @pl.when(me < NSP - 1)
    def _():
        halo_copy(me + 1).wait_recv()
        ext_ref[ROWS : ROWS + 32, :] = halo_ref[...]

    @pl.when(me == NSP - 1)
    def _():
        ext_ref[ROWS : ROWS + 32, :] = jnp.zeros((32, FG), f32)

    convolve(ROWS - 32, 32)

    whole = psi_ref.at[pl.ds(0, NSP // 2 - 1)]
    remote(whole, whole, psend.at[0], precv.at[0], me, right).wait_recv()
    for rt in range(4):
        for ct in range(2):
            total = psi_ref[0, rt * 2 + ct].astype(f32)
            for k in range(1, NSP // 2):
                total = total + psi_ref[k, rt * 2 + ct].astype(f32)
            owg_ref[rt * 16 : rt * 16 + 16, ct * 128 : ct * 128 + 128] = total

    @pl.when(me > 0)
    def _():
        halo_copy(me - 1).wait_send()

    remote(whole, whole, psend.at[0], precv.at[0], me, right).wait_send()
    remote(pin_ref, pin_ref, dsend.at[0], drecv.at[0], me, right).wait_send()
    for n in range(3):
        sent = stat_ref.at[n, pl.ds(1, NTP - 1)]
        remote(sent, sent, ssend.at[n], srecv.at[n], me, right).wait_send()
    for side in range(2):
        exchange(side).wait_send()
        gather(side, 0).wait_send()
        gather(side, 1).wait_send()
        gather_far(side).wait_send()
        sent = got_ref.at[:, pl.ds(0, NSP - WHOLE), side]
        remote(sent, sent, xfsend.at[side], xfrecv.at[0, side], me, right).wait_send()
        for g in range(NG):
            pair_copy(g, side).wait_send()
    for t in range(2):
        sent = send_ref.at[t, pl.ds(0, NSP - 1)]
        remote(sent, sent, fsend.at[t], frecv.at[t, 0], me, right).wait_send()
    sent = more_ref.at[:, pl.ds(0, WHOLE - 1)]
    remote(sent, sent, msend.at[0], mrecv.at[0, 0], me, right).wait_send()
    for g in range(NG):
        sent = back_ref.at[pl.ds(0, GB - 1 if g == 0 else GB)]
        remote(sent, sent, bsend.at[g], brecv.at[g], me, right).wait_send()
    for store in stores:
        store.wait()


def widen_kernel(*refs):
    half = len(refs) // 2
    for src, dst in zip(refs[:half], refs[half:]):
        dst[...] = src[...].astype(dst.dtype)


def on_device(
    expert_input,
    cotangent,
    routes,
    route_weight,
    expert_gate,
    expert_up,
    expert_down,
    conv_out,
    conv_value,
    conv_gate,
    conv_taps,
    norm_gain,
    norm_bias,
    out_weight,
):
    dma = pltpu.SemaphoreType.DMA
    vmem = pl.BlockSpec(memory_space=pltpu.VMEM)
    anywhere = pl.BlockSpec(memory_space=pl.ANY)
    shape = jax.ShapeDtypeStruct
    gate_grad, up_grad, down_grad, resid_grad, projected, value_grad, gate_in_grad = pl.pallas_call(
        layer_kernel,
        out_shape=(
            shape((D, FG), bf16),
            shape((D, FG), bf16),
            shape((FG, D), bf16),
            shape((ROWS, D), bf16),
            shape((OW, FG), f32),
            shape((ROWS, FG), bf16),
            shape((ROWS, FG), bf16),
        ),
        in_specs=[anywhere] * 9 + [vmem] * 5,
        out_specs=(anywhere,) * 4 + (vmem,) * 3,
        scratch_shapes=[
            pltpu.VMEM((ROWS, D), bf16),
            pltpu.VMEM((ROWS, D), bf16),
            pltpu.VMEM((D, FG), bf16),
            pltpu.VMEM((D, FG), bf16),
            pltpu.VMEM((FG, D), bf16),
            pltpu.VMEM((FG, D), bf16),
            pltpu.VMEM((ROWS, FG), bf16),
            pltpu.VMEM((ROWS, FG), bf16),
            pltpu.VMEM((ROWS, FG), bf16),
            pltpu.VMEM((D, FG), bf16),
            pltpu.VMEM((D, FG), bf16),
            pltpu.VMEM((FG, D), bf16),
            pltpu.VMEM((ROWS, D), bf16),
            pltpu.VMEM((NSP, ROWS), jnp.int32),
            pltpu.VMEM((NSP, ROWS), f32),
            pltpu.VMEM((NG * GO, ROWS), bf16),
            pltpu.VMEM((2, NSP, 2, NT, 16, 128), bf16),
            pltpu.VMEM((2, WHOLE, 2, NT, 16, 128), bf16),
            pltpu.VMEM((2, NSP, 4, NT, 16, 128), bf16),
            pltpu.VMEM((2, NSP * 36, D), bf16),
            pltpu.VMEM((3, NSP * 36, FG), bf16),
            pltpu.VMEM((4, NSP, NT, 16, 128), bf16),
            pltpu.VMEM((2, NSP, NT, 16, 128), bf16),
            pltpu.VMEM((NSP, 2, NT, 16, 128), bf16),
            pltpu.VMEM((NSP, 2, NT, 16, 128), bf16),
            pltpu.VMEM((ROWS, 2 * QW), f32),
            pltpu.VMEM((2, ROWS, 256), bf16),
            pltpu.VMEM((2, ROWS, 256), bf16),
            pltpu.VMEM((4, 2, ROWS, 256), bf16),
            pltpu.VMEM((3, NTP, 8, ROWS), f32),
            pltpu.VMEM((ROWS, FG), f32),
            pltpu.VMEM((ROWS, FG), f32),
            pltpu.VMEM((ROWS, FG), f32),
            pltpu.VMEM((ROWS, FG), bf16),
            pltpu.VMEM((ROWS + 32, FG), f32),
            pltpu.VMEM((32, FG), f32),
            pltpu.VMEM((NSP, 8, 16, 128), bf16),
            pltpu.VMEM((NSP // 2, 8, 16, 128), bf16),
            pltpu.VMEM((NSP // 2, 8, 16, 128), bf16),
            dma((9,)),
            dma((4,)),
            dma((2,)),
            dma((2, NSP)),
            dma((1,)),
            dma((2, WHOLE)),
            dma((2,)),
            dma((NG, 2)),
            dma((NG, 2)),
            dma((NG, 2)),
            dma((NG,)),
            dma((NG,)),
            dma((2,)),
            dma((2,)),
            dma((3, 2)),
            dma((3, 2)),
            dma((3,)),
            dma((3,)),
            dma((1,)),
            dma((1,)),
            dma((1,)),
            dma((1,)),
            dma((1,)),
            dma((4,)),
        ],
        compiler_params=pltpu.CompilerParams(
            collective_id=0, has_side_effects=True, vmem_limit_bytes=67000000
        ),
        name="layer",
    )(
        expert_input,
        cotangent,
        expert_gate[0],
        expert_up[0],
        expert_down[0],
        out_weight,
        conv_out,
        conv_value,
        conv_gate,
        routes.T,
        route_weight.T,
        conv_taps,
        norm_gain[None, :],
        norm_bias[None, :],
    )
    steps = 2

    def block(rows, cols):
        return pl.BlockSpec((rows // steps, cols), lambda n: (n, 0))

    sizes = [(D, FG), (D, FG), (FG, D), (ROWS, D), (OW, FG), (ROWS, FG), (ROWS, FG)]
    types = [f32, f32, f32, bf16, f32, bf16, bf16]
    gate_grad, up_grad, down_grad, resid_grad, projected, value_grad, gate_in_grad = pl.pallas_call(
        widen_kernel,
        grid=(steps,),
        out_shape=tuple(shape(size, kind) for size, kind in zip(sizes, types)),
        in_specs=[block(*size) for size in sizes],
        out_specs=tuple(block(*size) for size in sizes),
        name="widen",
    )(gate_grad, up_grad, down_grad, resid_grad, projected, value_grad, gate_in_grad)
    return (
        gate_grad[None],
        up_grad[None],
        down_grad[None],
        resid_grad,
        projected.T,
        value_grad,
        gate_in_grad,
    )


def solution(mesh):
    return jax.shard_map(
        on_device,
        mesh=mesh,
        in_specs=(
            P("sp", None),
            P("sp", None),
            P("sp", None),
            P("sp", None),
            P("sp", None, "tp"),
            P("sp", None, "tp"),
            P("sp", "tp", None),
            P("sp", "tp"),
            P("sp", "tp"),
            P("sp", "tp"),
            P(None, "tp"),
            P("tp"),
            P("tp"),
            P("tp", None),
        ),
        out_specs=(
            P("sp", None, "tp"),
            P("sp", None, "tp"),
            P("sp", "tp", None),
            P("sp", None),
            P("tp", "sp"),
            P("sp", "tp"),
            P("sp", "tp"),
        ),
        check_vma=False,
    )
```

```python
import jax
import jax.numpy as jnp
from jax import lax
from jax.experimental import pallas as pl
from jax.experimental.pallas import tpu as pltpu
from jax.sharding import PartitionSpec as P

MESH = pl.DeviceIdType.MESH
bf16 = jnp.bfloat16
f32 = jnp.float32
norm_eps = 1e-06

NSP = 32
NTP = 4
ROWS = 384
D = 2048
CH = 1024
KW = 31
QW = 512
FG = 256
NG = 8
GB = NSP // NG
GR = GB * 36
GM = GB * 32
GT = GB * 16
GO = GM + GT
NT = 9
WHOLE = 2
OW = D // NSP


def dot(a, b, ca=1, cb=0, precision=None):
    return lax.dot_general(
        a, b, (((ca,), (cb,)), ((), ())), preferred_element_type=f32, precision=precision
    )


def exact_dot(a, b, ca=1, cb=0):
    return dot(a, b, ca, cb, lax.Precision.HIGHEST)


def split(a):
    high = a.astype(bf16)
    return high, (a - high.astype(f32)).astype(bf16)


def row_sums(a):
    high, low = split(a)
    return dot(jnp.ones((8, 2 * FG), bf16), jnp.concatenate([high, low], axis=1), 1, 1)


def iota(shape, dim):
    return lax.broadcasted_iota(jnp.int32, shape, dim)


def at(start, size, step):
    return pl.ds(pl.multiple_of(start, step), size)


def layer_kernel(
    x_hbm,
    c_hbm,
    wg_hbm,
    wu_hbm,
    wd_hbm,
    ow_hbm,
    co_hbm,
    cv_hbm,
    cg_hbm,
    routes_ref,
    weight_ref,
    taps_ref,
    gain_ref,
    bias_ref,
    gg_hbm,
    ug_hbm,
    dg_hbm,
    resid_hbm,
    owg_ref,
    value_ref,
    gatein_ref,
    x_ref,
    c_ref,
    wg_ref,
    wu_ref,
    wd_ref,
    ow_ref,
    co_ref,
    cv_ref,
    cg_ref,
    gg_ref,
    ug_ref,
    dg_ref,
    resid_ref,
    rank_ref,
    wsel_ref,
    oh_ref,
    send_ref,
    more_ref,
    got_ref,
    rows_ref,
    hid_ref,
    part_ref,
    pair_ref,
    back_ref,
    home_ref,
    sum_ref,
    exo_ref,
    exi_ref,
    ag_ref,
    stat_ref,
    normed_ref,
    coef_ref,
    rstd_ref,
    act_ref,
    ext_ref,
    halo_ref,
    pso_ref,
    psi_ref,
    pin_ref,
    gates_ref,
    insem,
    outsem,
    fsend,
    frecv,
    msend,
    mrecv,
    xfsend,
    xfrecv,
    xbsend,
    xbrecv,
    bsend,
    brecv,
    esend,
    erecv,
    asend,
    arecv,
    ssend,
    srecv,
    hsend,
    hrecv,
    psend,
    precv,
    dsend,
    drecv,
):
    me = lax.axis_index("sp")
    x = lax.axis_index("tp")
    z, y, core = me // 8, (me // 2) % 4, me % 2
    right, left = (x + 1) % NTP, (x + 3) % NTP

    def offset(k):
        g, m = k // GB, k % GB
        lap, part = g * 4 // NG, g % (NG // 4)
        dz = part + (m // 2) * (NG // 4)
        return dz, (dz + lap) % 4, m % 2

    def peer_at(k):
        dz, dy, dc = offset(k)
        return ((z + dz) % 4) * 8 + ((y + dy) % 4) * 2 + (core + dc) % 2

    def source_at(k):
        dz, dy, dc = offset(k)
        return ((z + 4 - dz) % 4) * 8 + ((y + 4 - dy) % 4) * 2 + (core + dc) % 2

    def quarter(j):
        return (x + j) % NTP

    def remote(src, dst, send, recv, sp, tp):
        return pltpu.make_async_remote_copy(
            src_ref=src,
            dst_ref=dst,
            send_sem=send,
            recv_sem=recv,
            device_id=(sp, tp),
            device_id_type=MESH,
        )

    def to_left_or_right(side):
        return right if side else left

    loads = [
        pltpu.make_async_copy(src, dst, insem.at[n])
        for n, (src, dst) in enumerate(
            [
                (x_hbm, x_ref),
                (c_hbm, c_ref),
                (wg_hbm, wg_ref),
                (wu_hbm, wu_ref),
                (wd_hbm, wd_ref),
                (co_hbm, co_ref),
                (ow_hbm, ow_ref),
                (cv_hbm, cv_ref),
                (cg_hbm, cg_ref),
            ]
        )
    ]
    for load in loads:
        load.start()

    barrier = pltpu.get_barrier_semaphore()

    @pl.loop(1, NSP)
    def _(k):
        pl.semaphore_signal(barrier, inc=1, device_id=(peer_at(k), x), device_id_type=MESH)

    for j in range(1, NTP):
        pl.semaphore_signal(barrier, inc=1, device_id=(me, quarter(j)), device_id_type=MESH)

    r0, r1 = routes_ref[0:1, :], routes_ref[1:2, :]
    names = iota((NSP, ROWS), 0)
    m0, m1 = r0 == names, r1 == names
    member = jnp.where(m0 | m1, 1.0, 0.0).astype(bf16)
    before = jnp.where(iota((ROWS, ROWS), 0) < iota((ROWS, ROWS), 1), 1.0, 0.0).astype(bf16)
    rank = dot(member, before)
    rank_ref[...] = jnp.where(m0 | m1, rank, -1.0).astype(jnp.int32)
    wsel_ref[...] = jnp.where(m0, weight_ref[0:1, :], jnp.where(m1, weight_ref[1:2, :], 0.0))
    loads[0].wait()
    loads[1].wait()

    def forward_copy(t, k, peer):
        return remote(
            send_ref.at[t, k], got_ref.at[t, k, 0:2], fsend.at[t], frecv.at[t, k], peer, x
        )

    def more_copy(t, slot, k, peer):
        return remote(
            more_ref.at[t, slot], got_ref.at[t, k, 2:4], msend.at[0], mrecv.at[t, slot], peer, x
        )

    tile_col = (iota((GT, 128), 0) % 16) // 4

    def prepare(g):
        ohs, ws, ohrs, wrs = [], [], [], []
        for i in range(GB):
            peer = peer_at(g * GB + i)
            ranks = rank_ref[pl.ds(peer, 1), :]
            wsel = wsel_ref[pl.ds(peer, 1), :]
            one = ranks == iota((32, ROWS), 0)
            ohs.append(jnp.where(one, 1.0, 0.0).astype(bf16))
            ws.append(jnp.sum(jnp.where(one, wsel, 0.0), axis=1, keepdims=True))
            one = ranks == 32 + iota((16, ROWS), 0) % 4
            ohrs.append(jnp.where(one, 1.0, 0.0).astype(bf16))
            wrs.append(jnp.sum(jnp.where(one, wsel, 0.0), axis=1, keepdims=True))
        oh = jnp.concatenate(ohs + ohrs, axis=0)
        oh_ref[at(g * GO, GO, 16), :] = oh
        w = jnp.concatenate(ws + wrs, axis=0)
        def cut_tiles(t, j, store, members):
            ref = c_ref if t else x_ref
            main = dot(oh, ref[:, at(quarter(j) * QW, QW, QW)])
            if t:
                main = main * w
            rem = main[GM:]
            tail = jnp.zeros((GT, 128), f32)
            for cg in range(4):
                tail = jnp.where(tile_col == cg, rem[:, cg * 128 : (cg + 1) * 128], tail)
            main = main.astype(bf16)
            tail = tail.astype(bf16)
            for i in range(members):
                for rt in range(2):
                    for ct in range(4):
                        store(
                            i,
                            rt * 4 + ct,
                            main[
                                i * 32 + rt * 16 : i * 32 + rt * 16 + 16, ct * 128 : ct * 128 + 128
                            ],
                        )
                store(i, 8, tail[i * 16 : i * 16 + 16])

        def more(slot, members):
            for t in range(2):
                for j in range(2):

                    def store(i, tile, value):
                        more_ref[t, slot + i, j, tile] = value

                    cut_tiles(t, 2 + j, store, members)

        for t in range(2):
            for j in range(2):

                def store(i, tile, value):
                    send_ref[t, g * GB + i, j, tile] = value

                cut_tiles(t, j, store, GB)

        @pl.when(g == 0)
        def _():
            more(0, 2)

        @pl.when(g == 0)
        def _():
            pl.semaphore_wait(barrier, NSP - 1 + NTP - 1)
            for t in range(2):
                got_ref[t, 0, 0:2] = send_ref[t, 0]
                got_ref[t, 0, 2:4] = more_ref[t, 0]

        for t in range(2):
            for i in range(GB):
                k = g * GB + i

                @pl.when(k > 0)
                def _():
                    forward_copy(t, k, peer_at(k)).start()

                if i == 1:

                    @pl.when(g == 0)
                    def _():
                        more_copy(t, 1, k, peer_at(k)).start()

    ones = jnp.ones((8, FG), f32)
    spread = jnp.where(iota((8, 128), 0) == 0, 1.0, 0.0)
    spread1 = jnp.where(iota((8, 128), 0) == 1, 1.0, 0.0)

    def stat_copy(n, j):
        return remote(
            stat_ref.at[n, 0], stat_ref.at[n, NTP - j], ssend.at[n], srecv.at[n], me, quarter(j)
        )

    def stat_start(n, rows):
        stat_ref[n, 0] = rows
        for j in range(1, NTP):
            stat_copy(n, j).start()

    def stat_total(n):
        whole = stat_ref.at[n, pl.ds(1, NTP - 1)]
        remote(whole, whole, ssend.at[n], srecv.at[n], me, right).wait_recv()
        return (stat_ref[n, 0] + stat_ref[n, 1]) + (stat_ref[n, 2] + stat_ref[n, 3])

    def column(row_form, pick):
        high, low = split(row_form)
        low2 = (row_form - high.astype(f32) - low.astype(f32)).astype(bf16)
        terms = jnp.concatenate([high, low, low2, jnp.zeros_like(high)], axis=0)
        one = dot(terms, jnp.concatenate([pick] * 4, axis=0).astype(bf16), 0, 0)
        return jnp.concatenate([one, one], axis=1)


    def to_side(src, t, k, side):
        return remote(
            src,
            got_ref.at[t, k, 2 + side],
            xfsend.at[side],
            xfrecv.at[k // GB, side],
            me,
            to_left_or_right(side),
        )

    def pass_on(g):
        for t in range(2):

            @pl.loop(0, GB)
            def _(m):
                k = g * GB + m

                @pl.when(k > 0)
                def _():
                    forward_copy(t, k, source_at(k)).wait_recv()

                @pl.when(k > 1)
                def _():
                    to_side(got_ref.at[t, k, 0], t, k, 1).start()
                    to_side(got_ref.at[t, k, 1], t, k, 0).start()

    a = iota((GT, GT), 0)
    perm_col = (a % (GB * 4)) // 4 * 16 + (a // (GB * 4)) * 4 + a % 4
    perm = jnp.where(iota((GT, GT), 1) == perm_col, 1.0, 0.0).astype(bf16)

    def experts(g):
        base = g * GR
        first = g * GB
        def side_wait(start, size):
            for side in range(2):
                whole = got_ref.at[:, pl.ds(start, size), 2 + side]
                remote(
                    whole, whole, xfsend.at[side], xfrecv.at[g, side], me, to_left_or_right(side)
                ).wait_recv()

        @pl.when(g == 0)
        def _():
            side_wait(first + 2, GB - 2)

        @pl.when(g > 0)
        def _():
            side_wait(first, GB)

        @pl.when(g == 0)
        def _():
            for t in range(2):
                more_copy(t, 1, 1, source_at(1)).wait_recv()

        for t in range(2):
            for r in range(4):
                lane = quarter(r) * QW
                for i in range(GB):
                    for rt in range(2):
                        for ct in range(4):
                            rows_ref[
                                t,
                                at(base + i * 32 + rt * 16, 16, 16),
                                at(lane + ct * 128, 128, 128),
                            ] = got_ref[t, first + i, r, rt * 4 + ct]
                rem = dot(perm, got_ref[t, pl.ds(first, GB), r, 8].reshape(GT, 128)).astype(bf16)
                for cg in range(4):
                    rows_ref[
                        t, at(base + GM, GB * 4, 16), at(lane + cg * 128, 128, 128)
                    ] = rem[cg * GB * 4 : (cg + 1) * GB * 4]
        span = at(base, GR, 16)
        tok = rows_ref[0, span, :]
        pre_gate = dot(tok, wg_ref[...])
        pre_up = dot(tok, wu_ref[...])
        hidden_grad = dot(rows_ref[1, span, :], wd_ref[...], 1, 1)
        sig = jax.nn.sigmoid(pre_gate)
        act = pre_gate * sig
        hid_ref[0, span, :] = (act * pre_up).astype(bf16)
        gate_pre = (hidden_grad * pre_up * sig * (1.0 + pre_gate * (1.0 - sig))).astype(bf16)
        up_pre = (hidden_grad * act).astype(bf16)
        hid_ref[1, span, :] = gate_pre
        hid_ref[2, span, :] = up_pre
        for r in (2, 3, 0, 1):
            cols = at(quarter(r) * QW, QW, QW)
            part = dot(gate_pre, wg_ref[cols, :], 1, 1) + dot(up_pre, wu_ref[cols, :], 1, 1)
            part = part.astype(bf16)
            for i in range(GB):
                for rt in range(2):
                    for ct in range(4):
                        part_ref[r, first + i, rt * 4 + ct] = part[
                            i * 32 + rt * 16 : i * 32 + rt * 16 + 16, ct * 128 : ct * 128 + 128
                        ]
            stack = jnp.concatenate(
                [part[GM:GR, cg * 128 : cg * 128 + 128] for cg in range(4)], axis=0
            )
            rem = dot(perm, stack, 0, 0).astype(bf16)
            for i in range(GB):
                part_ref[r, first + i, 8] = rem[i * 16 : i * 16 + 16]
            if r >= 2:
                pair_copy(g, 3 - r).start()

    def pair_copy(g, side):
        group = pl.ds(g * GB, GB)
        return remote(
            part_ref.at[3 - side, group],
            pair_ref.at[side, group],
            xbsend.at[g, side],
            xbrecv.at[g, side],
            me,
            to_left_or_right(side),
        )

    def back_copy(g, m):
        k = g * GB + m
        return remote(
            back_ref.at[k], home_ref.at[k], bsend.at[g], brecv.at[g], source_at(k), x
        )

    def send_back(g):
        for side in range(2):
            pair_copy(g, side).wait_recv()

        @pl.loop(0, GB)
        def _(m):
            k = g * GB + m
            for j in range(2):
                both = part_ref[j, k].astype(f32) + pair_ref[j, k].astype(f32)
                back_ref[k, j] = both.astype(bf16)

            @pl.when(k > 0)
            def _():
                back_copy(g, m).start()

            @pl.when(k == 0)
            def _():
                home_ref[0] = back_ref[0]

    def home_wait(g):
        @pl.when(g == 0)
        def _():
            span = home_ref.at[pl.ds(1, GB - 1)]
            remote(span, span, bsend.at[g], brecv.at[g], peer_at(1), x).wait_recv()

        @pl.when(g > 0)
        def _():
            span = home_ref.at[pl.ds(g * GB, GB)]
            remote(span, span, bsend.at[g], brecv.at[g], peer_at(1), x).wait_recv()

    def combine(g, js=(0, 1)):
        oh = oh_ref[at(g * GO, GO, 16), :]
        for j in js:
            rows = []
            for i in range(GB):
                for rt in range(2):
                    rows.append(
                        jnp.concatenate(
                            [home_ref[g * GB + i, j, rt * 4 + ct] for ct in range(4)], axis=1
                        )
                    )
            rem = home_ref[pl.ds(g * GB, GB), j, 8].reshape(GT, 128).astype(f32)
            tails = [jnp.where(tile_col == cg, rem, 0.0).astype(bf16) for cg in range(4)]
            rows.append(jnp.concatenate(tails, axis=1))
            sum_ref[:, j * QW : (j + 1) * QW] += dot(oh, jnp.concatenate(rows, axis=0), 0, 0)

    sum_ref[...] = jnp.zeros_like(sum_ref)

    @pl.loop(0, NG)
    def _(g):
        prepare(g)

    @pl.loop(0, NG + 2)
    def _(step):
        @pl.when(step < NG)
        def _():
            pass_on(step)

        @pl.when(step == 0)
        def _():
            for load in loads[2:]:
                load.wait()
            stat_start(0, exact_dot(ones, co_ref[...].astype(f32), 1, 1))

        @pl.when(step == 5)
        def _():
            gate_sig = jax.nn.sigmoid(cg_ref[...].astype(f32))
            gates_ref[0] = gate_sig
            gates_ref[1] = cv_ref[...].astype(f32) * gate_sig * (1.0 - gate_sig)

        @pl.when(step == 2)
        def _():
            mean = column(stat_total(0), spread) / CH
            centred = co_ref[...].astype(f32) - mean
            normed_ref[...] = centred
            stat_start(1, exact_dot(ones, centred * centred, 1, 1))

        @pl.when(step == 4)
        def _():
            var = column(stat_total(1), spread) / CH
            rstd = lax.rsqrt(var + norm_eps)
            normed = normed_ref[...] * rstd
            norm_pre = normed * gain_ref[...] + bias_ref[...]
            norm_sig = jax.nn.sigmoid(norm_pre)
            act_ref[...] = (norm_pre * norm_sig).astype(bf16)
            normed_ref[...] = normed
            rstd_ref[...] = rstd
            coef_ref[...] = norm_sig * (1.0 + norm_pre * (1.0 - norm_sig)) * gain_ref[...]

        @pl.when((step > 0) & (step < NG + 1))
        def _():
            experts(step - 1)

        @pl.when(step > 1)
        def _():
            send_back(step - 2)

    def weight_grads(g):
        cols = pl.ds(g * QW, QW)
        tok = rows_ref[0, :, cols]
        gg_ref[cols, :] = dot(tok, hid_ref[1], 0, 0).astype(bf16)
        ug_ref[cols, :] = dot(tok, hid_ref[2], 0, 0).astype(bf16)
        dg_ref[:, cols] = dot(hid_ref[0], rows_ref[1, :, cols], 0, 0).astype(bf16)

    stores = [
        pltpu.make_async_copy(src, dst, outsem.at[n])
        for n, (src, dst) in enumerate(
            [(gg_ref, gg_hbm), (ug_ref, ug_hbm), (dg_ref, dg_hbm), (resid_ref, resid_hbm)]
        )
    ]
    weight_grads(0)

    @pl.loop(0, NG - 1)
    def _(g):
        home_wait(g)
        combine(g)

    home_wait(NG - 1)
    def exchange(side):
        return remote(
            exo_ref.at[side],
            exi_ref.at[side],
            esend.at[side],
            erecv.at[side],
            me,
            to_left_or_right(side),
        )

    combine(NG - 1, (1,))
    exo_ref[1] = sum_ref[:, QW : QW + 256].astype(bf16)
    exchange(1).start()
    combine(NG - 1, (0,))
    exo_ref[0] = sum_ref[:, 256:QW].astype(bf16)
    exchange(0).start()
    weight_grads(1)
    weight_grads(2)
    for side in range(2):
        exchange(side).wait_recv()
    cot0 = c_ref[:, at(quarter(0) * QW, 256, 256)].astype(f32)
    cot1 = c_ref[:, at(quarter(1) * QW + 256, 256, 256)].astype(f32)
    ag_ref[0, 0] = (cot0 + (sum_ref[:, :256] + exi_ref[1].astype(f32))).astype(bf16)
    ag_ref[0, 1] = (cot1 + (sum_ref[:, QW + 256 :] + exi_ref[0].astype(f32))).astype(bf16)

    def gather(side, part):
        return remote(
            ag_ref.at[0, part],
            ag_ref.at[3 if side else 1, part],
            asend.at[side, part],
            arecv.at[side, part],
            me,
            to_left_or_right(side),
        )

    def gather_far(side):
        return remote(
            ag_ref.at[3 if side else 1, 1 - side],
            ag_ref.at[2, 1 - side],
            asend.at[2, side],
            arecv.at[2, side],
            me,
            to_left_or_right(side),
        )

    def place(o, part):
        cols = at(quarter(o + part) * QW + part * 256, 256, 256)
        resid_ref[:, cols] = ag_ref[o, part]
        return dot(ag_ref[o, part], ow_ref[:, cols], 1, 1)

    def owner(o, part, i):
        return quarter(o + part) * 8 + part * 4 + i

    def partner_copy(o, peer):
        return remote(
            pso_ref.at[peer],
            pin_ref.at[peer // 2],
            dsend.at[0],
            drecv.at[o],
            (me // 2) * 2 + 1 - core,
            x,
        )

    def owg_copy(peer):
        return remote(
            pso_ref.at[peer], psi_ref.at[me // 2], psend.at[0], precv.at[0], peer, x
        )

    def project(o, part):
        term = dot(ag_ref[o, part], act_ref[...], 0, 0).astype(bf16)
        for i in range(4):
            for rt in range(4):
                for ct in range(2):
                    pso_ref[owner(o, part, i), rt * 2 + ct] = term[
                        i * OW + rt * 16 : i * OW + rt * 16 + 16, ct * 128 : ct * 128 + 128
                    ]
        for i in range(2):
            partner_copy(o, owner(o, part, 2 * i + 1 - core)).start()

    def relay(o):
        four = pin_ref.at[pl.ds(0, 4)]
        remote(four, four, dsend.at[0], drecv.at[o], me, right).wait_recv()
        for part in range(2):
            for i in range(2):
                peer = owner(o, part, 2 * i + core)
                both = pso_ref[peer].astype(f32) + pin_ref[peer // 2].astype(f32)
                pso_ref[peer] = both.astype(bf16)

                @pl.when(peer == me)
                def _():
                    psi_ref[me // 2] = pso_ref[me]

                @pl.when(peer != me)
                def _():
                    owg_copy(peer).start()

    for side in range(2):
        gather(side, 1 - side).start()
    for side in range(2):
        gather(side, side).start()
    mix_grad = place(0, 0) + place(0, 1)
    project(0, 0)
    project(0, 1)
    weight_grads(3)
    for store in stores[:3]:
        store.start()
    for side in range(2):
        gather(side, 1 - side).wait_recv()
        gather_far(side).start()
    mix_grad = mix_grad + place(1, 1) + place(3, 0)
    relay(0)
    project(1, 1)
    project(3, 0)
    for side in range(2):
        gather(side, side).wait_recv()
    mix_grad = mix_grad + place(1, 0) + place(3, 1)
    project(1, 0)
    project(3, 1)
    relay(1)
    relay(3)
    for side in range(2):
        gather_far(side).wait_recv()
    mix_grad = mix_grad + place(2, 0) + place(2, 1)
    stores[3].start()

    norm_grad = mix_grad * coef_ref[...]
    sum_rows = row_sums(norm_grad)
    dot_rows = row_sums(norm_grad * normed_ref[...])
    stat_start(2, jnp.where(iota((8, ROWS), 0) == 0, sum_rows, dot_rows))

    project(2, 0)
    project(2, 1)
    relay(2)
    totals = stat_total(2)
    conv_grad = rstd_ref[...] * (
        norm_grad
        - column(totals, spread) / CH
        - normed_ref[...] * (column(totals, spread1) / CH)
    )
    ext_ref[0:ROWS, :] = conv_grad

    def halo_copy(sp):
        return remote(ext_ref.at[0:32], halo_ref, hsend.at[0], hrecv.at[0], sp, x)

    @pl.when(me > 0)
    def _():
        halo_copy(me - 1).start()

    def convolve(start, rows):
        glu = jnp.zeros((rows, FG), f32)
        for lag in range(KW):
            begin = start + KW - 1 - lag
            glu = glu + taps_ref[lag : lag + 1, :] * ext_ref[begin : begin + rows, :]
        span = pl.ds(start, rows)
        value_ref[span, :] = (glu * gates_ref[0, span, :]).astype(bf16)
        gatein_ref[span, :] = (glu * gates_ref[1, span, :]).astype(bf16)

    for start in range(0, ROWS - 32, 32):
        convolve(start, 32)

    @pl.when(me < NSP - 1)
    def _():
        halo_copy(me + 1).wait_recv()
        ext_ref[ROWS : ROWS + 32, :] = halo_ref[...]

    @pl.when(me == NSP - 1)
    def _():
        ext_ref[ROWS : ROWS + 32, :] = jnp.zeros((32, FG), f32)

    convolve(ROWS - 32, 32)

    whole = psi_ref.at[pl.ds(0, NSP // 2 - 1)]
    remote(whole, whole, psend.at[0], precv.at[0], me, right).wait_recv()
    for rt in range(4):
        for ct in range(2):
            total = psi_ref[0, rt * 2 + ct].astype(f32)
            for k in range(1, NSP // 2):
                total = total + psi_ref[k, rt * 2 + ct].astype(f32)
            owg_ref[rt * 16 : rt * 16 + 16, ct * 128 : ct * 128 + 128] = total

    @pl.when(me > 0)
    def _():
        halo_copy(me - 1).wait_send()

    remote(whole, whole, psend.at[0], precv.at[0], me, right).wait_send()
    remote(pin_ref, pin_ref, dsend.at[0], drecv.at[0], me, right).wait_send()
    for n in range(3):
        sent = stat_ref.at[n, pl.ds(1, NTP - 1)]
        remote(sent, sent, ssend.at[n], srecv.at[n], me, right).wait_send()
    for side in range(2):
        exchange(side).wait_send()
        gather(side, 0).wait_send()
        gather(side, 1).wait_send()
        gather_far(side).wait_send()
        sent = got_ref.at[:, pl.ds(0, NSP - WHOLE), side]
        remote(sent, sent, xfsend.at[side], xfrecv.at[0, side], me, right).wait_send()
        for g in range(NG):
            pair_copy(g, side).wait_send()
    for t in range(2):
        sent = send_ref.at[t, pl.ds(0, NSP - 1)]
        remote(sent, sent, fsend.at[t], frecv.at[t, 0], me, right).wait_send()
    sent = more_ref.at[:, pl.ds(0, WHOLE - 1)]
    remote(sent, sent, msend.at[0], mrecv.at[0, 0], me, right).wait_send()
    for g in range(NG):
        sent = back_ref.at[pl.ds(0, GB - 1 if g == 0 else GB)]
        remote(sent, sent, bsend.at[g], brecv.at[g], me, right).wait_send()
    for store in stores:
        store.wait()


def widen_kernel(*refs):
    half = len(refs) // 2
    for src, dst in zip(refs[:half], refs[half:]):
        dst[...] = src[...].astype(dst.dtype)


def on_device(
    expert_input,
    cotangent,
    routes,
    route_weight,
    expert_gate,
    expert_up,
    expert_down,
    conv_out,
    conv_value,
    conv_gate,
    conv_taps,
    norm_gain,
    norm_bias,
    out_weight,
):
    dma = pltpu.SemaphoreType.DMA
    vmem = pl.BlockSpec(memory_space=pltpu.VMEM)
    anywhere = pl.BlockSpec(memory_space=pl.ANY)
    shape = jax.ShapeDtypeStruct
    gate_grad, up_grad, down_grad, resid_grad, projected, value_grad, gate_in_grad = pl.pallas_call(
        layer_kernel,
        out_shape=(
            shape((D, FG), bf16),
            shape((D, FG), bf16),
            shape((FG, D), bf16),
            shape((ROWS, D), bf16),
            shape((OW, FG), f32),
            shape((ROWS, FG), bf16),
            shape((ROWS, FG), bf16),
        ),
        in_specs=[anywhere] * 9 + [vmem] * 5,
        out_specs=(anywhere,) * 4 + (vmem,) * 3,
        scratch_shapes=[
            pltpu.VMEM((ROWS, D), bf16),
            pltpu.VMEM((ROWS, D), bf16),
            pltpu.VMEM((D, FG), bf16),
            pltpu.VMEM((D, FG), bf16),
            pltpu.VMEM((FG, D), bf16),
            pltpu.VMEM((FG, D), bf16),
            pltpu.VMEM((ROWS, FG), bf16),
            pltpu.VMEM((ROWS, FG), bf16),
            pltpu.VMEM((ROWS, FG), bf16),
            pltpu.VMEM((D, FG), bf16),
            pltpu.VMEM((D, FG), bf16),
            pltpu.VMEM((FG, D), bf16),
            pltpu.VMEM((ROWS, D), bf16),
            pltpu.VMEM((NSP, ROWS), jnp.int32),
            pltpu.VMEM((NSP, ROWS), f32),
            pltpu.VMEM((NG * GO, ROWS), bf16),
            pltpu.VMEM((2, NSP, 2, NT, 16, 128), bf16),
            pltpu.VMEM((2, WHOLE, 2, NT, 16, 128), bf16),
            pltpu.VMEM((2, NSP, 4, NT, 16, 128), bf16),
            pltpu.VMEM((2, NSP * 36, D), bf16),
            pltpu.VMEM((3, NSP * 36, FG), bf16),
            pltpu.VMEM((4, NSP, NT, 16, 128), bf16),
            pltpu.VMEM((2, NSP, NT, 16, 128), bf16),
            pltpu.VMEM((NSP, 2, NT, 16, 128), bf16),
            pltpu.VMEM((NSP, 2, NT, 16, 128), bf16),
            pltpu.VMEM((ROWS, 2 * QW), f32),
            pltpu.VMEM((2, ROWS, 256), bf16),
            pltpu.VMEM((2, ROWS, 256), bf16),
            pltpu.VMEM((4, 2, ROWS, 256), bf16),
            pltpu.VMEM((3, NTP, 8, ROWS), f32),
            pltpu.VMEM((ROWS, FG), f32),
            pltpu.VMEM((ROWS, FG), f32),
            pltpu.VMEM((ROWS, FG), f32),
            pltpu.VMEM((ROWS, FG), bf16),
            pltpu.VMEM((ROWS + 32, FG), f32),
            pltpu.VMEM((32, FG), f32),
            pltpu.VMEM((NSP, 8, 16, 128), bf16),
            pltpu.VMEM((NSP // 2, 8, 16, 128), bf16),
            pltpu.VMEM((NSP // 2, 8, 16, 128), bf16),
            pltpu.VMEM((2, ROWS, FG), f32),
            dma((9,)),
            dma((4,)),
            dma((2,)),
            dma((2, NSP)),
            dma((1,)),
            dma((2, WHOLE)),
            dma((2,)),
            dma((NG, 2)),
            dma((NG, 2)),
            dma((NG, 2)),
            dma((NG,)),
            dma((NG,)),
            dma((2,)),
            dma((2,)),
            dma((3, 2)),
            dma((3, 2)),
            dma((3,)),
            dma((3,)),
            dma((1,)),
            dma((1,)),
            dma((1,)),
            dma((1,)),
            dma((1,)),
            dma((4,)),
        ],
        compiler_params=pltpu.CompilerParams(
            collective_id=0, has_side_effects=True, vmem_limit_bytes=67000000
        ),
        name="layer",
    )(
        expert_input,
        cotangent,
        expert_gate[0],
        expert_up[0],
        expert_down[0],
        out_weight,
        conv_out,
        conv_value,
        conv_gate,
        routes.T,
        route_weight.T,
        conv_taps,
        norm_gain[None, :],
        norm_bias[None, :],
    )
    steps = 2

    def block(rows, cols):
        return pl.BlockSpec((rows // steps, cols), lambda n: (n, 0))

    sizes = [(D, FG), (D, FG), (FG, D), (ROWS, D), (OW, FG), (ROWS, FG), (ROWS, FG)]
    types = [f32, f32, f32, bf16, f32, bf16, bf16]
    gate_grad, up_grad, down_grad, resid_grad, projected, value_grad, gate_in_grad = pl.pallas_call(
        widen_kernel,
        grid=(steps,),
        out_shape=tuple(shape(size, kind) for size, kind in zip(sizes, types)),
        in_specs=[block(*size) for size in sizes],
        out_specs=tuple(block(*size) for size in sizes),
        name="widen",
    )(gate_grad, up_grad, down_grad, resid_grad, projected, value_grad, gate_in_grad)
    return (
        gate_grad[None],
        up_grad[None],
        down_grad[None],
        resid_grad,
        projected.T,
        value_grad,
        gate_in_grad,
    )


def solution(mesh):
    return jax.shard_map(
        on_device,
        mesh=mesh,
        in_specs=(
            P("sp", None),
            P("sp", None),
            P("sp", None),
            P("sp", None),
            P("sp", None, "tp"),
            P("sp", None, "tp"),
            P("sp", "tp", None),
            P("sp", "tp"),
            P("sp", "tp"),
            P("sp", "tp"),
            P(None, "tp"),
            P("tp"),
            P("tp"),
            P("tp", None),
        ),
        out_specs=(
            P("sp", None, "tp"),
            P("sp", None, "tp"),
            P("sp", "tp", None),
            P("sp", None),
            P("tp", "sp"),
            P("sp", "tp"),
            P("sp", "tp"),
        ),
        check_vma=False,
    )
```
